32 devices in a mesh: grp: 2 (over y), ep: 4 (over z), tp: 4 (over x, core).
Axes of the slice: x: 2, y: 2, z: 4, core: 2. Of those that a mesh axis runs over, the one named last changes fastest.
Arguments:
- tokens: bfloat16 [4096, 2048], P(('grp', 'ep', 'tp')), parts along dimension 0, may hold values from -6 to 6
- norm_gain: float32 [2048], replicated, may hold values from 0.1 to 1.9
- route_ids: int32 [4096, 2], P(('grp', 'ep', 'tp')), parts along dimension 0, may hold values from 0 to 15, all different within a row; in each aligned block of 128 rows (0 to 127, 128 to 255, ...) at most 24 rows name the same one
- route_weights: float32 [4096, 2], P(('grp', 'ep', 'tp')), parts along dimension 0, may hold values from 0.1 to 0.9
- w_gate: bfloat16 [16, 2048, 512], P(('ep', 'tp')), may hold values from -0.125 to 0.125
- w_up: bfloat16 [16, 2048, 512], P(('ep', 'tp')), may hold values from -0.125 to 0.125
- w_down: bfloat16 [16, 512, 2048], P(('ep', 'tp')), may hold values from -0.25 to 0.25
Outputs:
- mixed: bfloat16 [4096, 2048], P(('grp', 'ep', 'tp')), parts along dimension 0
The draws below stay inside these ranges and needn't reach their ends.
There are 2 independent parts, one for each index of `grp`. The reference program is written for one: setup_inputs(seed, part) draws one part's arguments, and reference() takes and returns one part's arrays. A program takes and returns all parts, laid end to end along the dimension named above; an argument that names none is the same for every part. Nothing has to cross between parts.
Inputs may be any that keep to these rules, and one draw needn't show every extreme that they name: `route_ids`: each token names 2 different experts. Among the tokens of one device (aligned blocks of 128 tokens) no expert is named more than 24 times, a bound that some block reaches.
All inputs are finite; a program needn't handle non-finite values.
Results may differ from the reference program's by a relative error of at most 0.0071.
Values may be sent and summed in bfloat16 or wider, within the bound.
A program may use at most 64 MiB of HBM per device.

```python
import math
import jax
import jax.numpy as jnp
import numpy as np
from jax import lax

D = 2048
FF = 512
TOP = 2
TOK_DEV = 128
EXPERTS = 16
CAP = 24
TOKENS = 2048


def block_scale(own_key, shape, shards, least, high):
    loudness, own = 1.0, jax.random.fold_in(own_key, 6)
    for dim, shards_of in shards:
        heights = jnp.exp(jax.random.uniform(jax.random.fold_in(own, dim), (shards_of,), jnp.float32, least / len(shards), high / len(shards)))
        loudness = loudness * jnp.repeat(heights, shape[dim] // shards_of).reshape([-1 if axis == dim else 1 for axis in range(len(shape))])
    return loudness


def routed_block(key, own, number, rows, amount, top, limit, skew):
    order = jax.random.permutation(key, amount)
    packed, ordinary = load_shares(amount, rows * top, limit, skew, True), load_shares(amount, rows * top, limit, skew, False)
    places = jnp.arange(amount)

    def named(lengths, turn):
        used = int((lengths > 0).sum())
        fixed = max(1, used // 4)
        shifted = fixed + (places - fixed + turn * (used - fixed)) % max(1, amount - fixed)
        return jnp.zeros((amount,), jnp.int32).at[order[jnp.where(places < fixed, places, shifted)]].set(jnp.asarray(lengths, jnp.int32))

    lengths = jnp.where(number % 4 == 0, named(packed, number // 4), named(ordinary, number - number // 4 - 1))
    mixed = jax.random.permutation(jax.random.fold_in(own, 3), amount)
    source_of, sink = mixed[0:amount // 2 * 2:2], mixed[1:amount // 2 * 2:2]
    slack = jnp.minimum(lengths[source_of] - 1, limit - lengths[sink]) // 2
    slack = jnp.where((source_of == order[0]) | (sink == order[0]) | (lengths[sink] == 0), 0, jnp.maximum(slack, 0))
    shifted = jax.random.randint(jax.random.fold_in(own, 4), (amount // 2,), 0, 1 << 20) % (slack + 1)
    lengths = lengths.at[source_of].add(-shifted).at[sink].add(shifted)
    labels = jnp.searchsorted(jnp.cumsum(lengths), jnp.arange(rows * top), side="right").astype(jnp.int32)
    table = labels.reshape(top, rows).T
    table = table[jax.random.permutation(jax.random.fold_in(own, 1), rows)]
    turn = jax.random.randint(jax.random.fold_in(own, 2), (rows, 1), 0, top)
    return jnp.take_along_axis(table, (jnp.arange(top)[None, :] + turn) % top, axis=1)


def load_shares(number_of, total, most, lean, full):
    portions = [(1 << 20) // math.isqrt(rank ** lean) + 1 for rank in range(1, number_of + 1)]
    largest = most if full else min(most, max(-(-total // number_of), total * portions[0] // sum(portions)))
    least = 1 if total - largest >= number_of - 1 else 0
    holding, surplus = [largest] + [least] * (number_of - 1), total - largest - least * (number_of - 1)
    while surplus > 0:
        movable = [i for i in range(1, number_of) if holding[i] < largest] or [i for i in range(1, number_of) if holding[i] < most]
        pool, left = sum([portions[i] for i in movable]), surplus
        for i in movable:
            more = min(most - holding[i], max(1, left * portions[i] // pool), surplus)
            holding[i] = holding[i] + more
            surplus = surplus - more
    return np.array(holding)


def centred(stream_key, extent, deviation, most, pieces=(), kind=jnp.bfloat16):
    loudness = block_scale(stream_key, extent, pieces, -0.22, 0.18) if pieces else 1.0
    values = jax.random.normal(stream_key, extent, jnp.float32) * deviation * loudness
    return jnp.minimum(jnp.maximum(values, -most), most).astype(kind)


def setup_inputs(seed: int = 0, part: int = 0) -> dict:
    key_list = jax.random.split(jax.random.key(seed), 8)
    own_keys = jax.random.split(jax.random.fold_in(key_list[7], part), 8)
    tokens = centred(own_keys[0], (TOKENS, D), 1.0, 6.0, ((0, 16),))
    norm_gain = jnp.clip(1.0 + 0.18 * jax.random.normal(key_list[1], (D,), jnp.float32), 0.1, 1.9)
    route_ids_keys = jax.random.split(jax.random.fold_in(own_keys[2], 1), TOKENS // TOK_DEV)
    route_ids_turns = jax.random.permutation(jax.random.fold_in(own_keys[2], 3), TOKENS // TOK_DEV)
    route_ids = jax.vmap(lambda own, number: routed_block(jax.random.fold_in(own_keys[2], 2), own, number, TOK_DEV, EXPERTS, TOP, CAP, 2))(route_ids_keys, route_ids_turns).reshape((TOKENS, TOP))
    route_weights = jnp.clip(0.1 + 0.79999997 * jax.random.uniform(own_keys[3], (TOKENS, TOP), jnp.float32) ** block_scale(own_keys[3], (TOKENS, TOP), ((0, 16),), -0.2, 0.2), 0.1, 0.9)
    w_gate = centred(key_list[4], (EXPERTS, D, FF), D ** -0.5, 0.125, ((0, 16),))
    w_up = centred(key_list[5], (EXPERTS, D, FF), D ** -0.5, 0.125, ((0, 16),))
    w_down = centred(key_list[6], (EXPERTS, FF, D), FF ** -0.5, 0.25, ((0, 16),))
    return {"tokens": tokens, "norm_gain": norm_gain, "route_ids": route_ids, "route_weights": route_weights, "w_gate": w_gate, "w_up": w_up, "w_down": w_down}


def reference(tokens, norm_gain, route_ids, route_weights, w_gate, w_up, w_down):
    source_count = TOKENS // TOK_DEV
    values = tokens.astype(jnp.float32)
    normed = (values * lax.rsqrt(lax.optimization_barrier(jnp.mean(values * values, axis=-1, keepdims=True)) + 1e-06) * norm_gain).astype(jnp.bfloat16)
    per_device = route_ids.reshape(source_count, TOK_DEV * TOP)
    onehot = (per_device[:, :, None] == jnp.arange(EXPERTS, dtype=jnp.int32)[None, None, :]).astype(jnp.int32)
    slot_index = lax.optimization_barrier(jnp.sum((jnp.cumsum(onehot, axis=1) - onehot) * onehot, axis=-1))
    position = (jnp.arange(source_count, dtype=jnp.int32)[:, None] * CAP + slot_index).reshape(-1).astype(jnp.int32)
    flat_ids = route_ids.reshape(-1)
    total_rows = TOKENS * TOP
    row_table = jnp.full((EXPERTS, source_count * CAP), total_rows, jnp.int32)
    row_table = row_table.at[flat_ids, position].set(jnp.arange(total_rows, dtype=jnp.int32))

    def apply_expert(carry, operand):
        table_row, gate_w, up_w, down_w = operand
        token_rows = normed[jnp.minimum(table_row // TOP, TOKENS - 1)]
        gate_act = jnp.dot(token_rows, gate_w, preferred_element_type=jnp.float32)
        up_act = jnp.dot(token_rows, up_w, preferred_element_type=jnp.float32)
        hidden = (jax.nn.silu(gate_act) * up_act).astype(jnp.bfloat16)
        result = jnp.dot(hidden, down_w, preferred_element_type=jnp.float32).astype(jnp.bfloat16)
        return (carry.at[table_row].set(result), None)
    start = jnp.zeros((total_rows + 1, D), jnp.bfloat16)
    picked, _ = lax.scan(apply_expert, start, (row_table, w_gate, w_up, w_down))
    picked = picked[:total_rows].reshape(TOKENS, TOP, D).astype(jnp.float32)
    return lax.optimization_barrier(jnp.sum(picked * route_weights[:, :, None], axis=1)).astype(jnp.bfloat16)
```

```python
import functools

import jax
import jax.numpy as jnp
from jax import lax
from jax.experimental import pallas as pl
from jax.experimental.pallas import tpu as pltpu
from jax.sharding import PartitionSpec as P

MESH = pl.DeviceIdType.MESH


def plain(tokens, norm_gain, route_ids, route_weights, w_gate, w_up, w_down):
    tok_rows, model_width = tokens.shape
    top_count = route_ids.shape[1]
    ep_count = lax.axis_size("ep")
    tp_count = lax.axis_size("tp")
    experts = ep_count * tp_count
    capacity = 3 * tok_rows * top_count // (2 * experts)
    values = tokens.astype(jnp.float32)
    normed = (
        values * lax.rsqrt(jnp.mean(values * values, axis=-1, keepdims=True) + 1e-06) * norm_gain
    ).astype(jnp.bfloat16)
    flat_ids = route_ids.reshape(-1)
    onehot = (flat_ids[:, None] == jnp.arange(experts, dtype=jnp.int32)[None, :]).astype(jnp.int32)
    slot_index = jnp.sum((jnp.cumsum(onehot, axis=0) - onehot) * onehot, axis=-1)
    token_of = jnp.arange(tok_rows * top_count, dtype=jnp.int32) // top_count
    buffer = jnp.zeros((experts, capacity, model_width), jnp.bfloat16)
    buffer = buffer.at[flat_ids, slot_index].set(normed[token_of])
    received = lax.all_to_all(buffer, ("ep", "tp"), split_axis=0, concat_axis=0, tiled=True)
    flat_rows = received.reshape(-1, model_width)
    gate_act = jnp.dot(flat_rows, w_gate[0], preferred_element_type=jnp.float32)
    up_act = jnp.dot(flat_rows, w_up[0], preferred_element_type=jnp.float32)
    hidden = (jax.nn.silu(gate_act) * up_act).astype(jnp.bfloat16)
    result = jnp.dot(hidden, w_down[0], preferred_element_type=jnp.float32).astype(jnp.bfloat16)
    returned = lax.all_to_all(
        result.reshape(received.shape), ("ep", "tp"), split_axis=0, concat_axis=0, tiled=True
    )
    picked = (
        returned[flat_ids, slot_index].reshape(tok_rows, top_count, model_width).astype(jnp.float32)
    )
    return jnp.sum(picked * route_weights[:, :, None], axis=1).astype(jnp.bfloat16)


def flipped(index, bits):
    bit = 1
    while bit <= bits:
        if bits & bit:
            index = index + (1 - 2 * ((index // bit) % 2)) * bit
        bit *= 2
    return index


PIECES = 4
EARLY = 4


def kernel(
    ep_count, tp_count, cap,
    x_hbm, gain_ref, ids_ref, wts_ref, wg_hbm, wu_hbm, wd_hbm, out_hbm,
    x_ref, out_ref, io_sem,
    normed, meta, share_hi, share_lo, nsend, nrecv, nres, nback,
    eblock, emeta, epick, esend,
    rblock, rmeta, rpick, rshare_hi, rshare_lo, fsend, frecv, fres, rback, rsend, farback,
    wg, wu, wd, acc, gate_acc, up_acc,
    w_sem, dense_s, fwd_s, edense_r, dense_r, meta_s, emeta_r, meta_r, near_s, near_r,
    eout_s, nret_s, nret_r, far_s, far_r, fret_s, fret_r, final_s, final_r,
):
    ep, tp, grp = lax.axis_index("ep"), lax.axis_index("tp"), lax.axis_index("grp")
    rows, width = x_ref.shape
    part_w = width // PIECES
    top = ids_ref.shape[0]
    experts = ep_count * tp_count
    near = 2 * tp_count
    me = ep * tp_count + tp
    boundary = (ep + ep // 2) % 2
    place_of_me = (1 - boundary) * tp_count
    own_relay = 1 + ep // 2
    is_boundary, is_end = boundary == 1, boundary == 0

    def at(plane, j):
        return (grp, plane, flipped(tp, j))

    def remote(src, dst, s_sem, r_sem, target):
        return pltpu.make_async_remote_copy(
            src_ref=src, dst_ref=dst, send_sem=s_sem, recv_sem=r_sem,
            device_id=target, device_id_type=MESH,
        )

    barrier = pltpu.get_barrier_semaphore()

    def greet(target):
        pl.semaphore_signal(barrier, inc=1, device_id=target, device_id_type=MESH)

    greet(at(flipped(ep, 2), 0))

    @pl.when(is_boundary)
    def _():
        greet(at(flipped(ep, 3), 0))

    for g in range(near - 1, 0, -1):
        greet(at(flipped(ep, g // tp_count), g % tp_count))
    fetch = pltpu.make_async_copy(x_hbm, x_ref, io_sem.at[0])
    fetch.start()
    loads = [
        pltpu.make_async_copy(src.at[0], dst, w_sem.at[i])
        for i, (src, dst) in enumerate(((wg_hbm, wg), (wu_hbm, wu), (wd_hbm, wd)))
    ]
    for load in loads:
        load.start()

    partner, across_mid = flipped(ep, 1), flipped(ep, 3)
    planes = [ep, partner]
    dense = [
        remote(normed.at[c], rblock.at[0, c], dense_s.at[c], dense_r.at[0, c], at(across_mid, 0))
        for c in range(PIECES)
    ]
    forward = [
        remote(eblock.at[c], rblock.at[1, c], fwd_s.at[c], dense_r.at[1, c], at(across_mid, 0))
        for c in range(PIECES)
    ]
    edense = [
        remote(normed.at[c], eblock.at[c], dense_s.at[c], edense_r.at[c], at(partner, 0))
        for c in range(PIECES)
    ]
    far_meta = pl.ds(0, 2 * near)
    meta_copy = remote(meta.at[far_meta], rmeta.at[0], meta_s.at[0], meta_r.at[0],
                       at(across_mid, 0))
    meta_forward = remote(emeta.at[far_meta], rmeta.at[1], meta_s.at[1], meta_r.at[1],
                          at(across_mid, 0))
    emeta_copy = remote(meta, emeta, meta_s.at[0], emeta_r.at[0], at(partner, 0))
    stores = [
        pltpu.make_async_copy(
            out_ref.at[:, pl.ds(c * part_w, part_w)], out_hbm.at[:, pl.ds(c * part_w, part_w)],
            io_sem.at[1 + c])
        for c in range(PIECES)
    ]
    near_out = [
        remote(nsend.at[g], nrecv.at[g], near_s.at[g], near_r.at[g],
               at(planes[g // tp_count], g % tp_count))
        for g in range(near)
    ]
    eout = [
        remote(esend.at[j], nrecv.at[tp_count + j], eout_s.at[j], near_r.at[tp_count + j],
               at(ep, j))
        for j in range(tp_count)
    ]
    near_ret = [
        remote(nres.at[g], nback.at[g], nret_s.at[g], nret_r.at[g],
               at(planes[g // tp_count], g % tp_count))
        for g in range(near)
    ]
    far_out, far_ret, final = {}, {}, {}
    for v in range(2):
        for c in range(PIECES):
            for i in range(near):
                far_out[v, c, i] = remote(
                    fsend.at[v, c, i], frecv.at[v, c, i % tp_count], far_s.at[v, c, i],
                    far_r.at[v, c, i % tp_count], at(planes[i // tp_count], i % tp_count))
            for j in range(tp_count):
                place = place_of_me + j
                far_ret[v, c, j] = remote(
                    fres.at[v, c, j], rback.at[v, c, place], fret_s.at[v, c, j],
                    fret_r.at[v, c, place], at(own_relay, j))
            final[v, c] = remote(rsend.at[v, c], farback.at[c], final_s.at[v, c], final_r.at[c],
                                 at(flipped(ep, 3 - v), 0))

    down = lax.broadcasted_iota(jnp.int32, (rows, rows), 0)
    across = lax.broadcasted_iota(jnp.int32, (rows, rows), 1)

    expert_of = lax.broadcasted_iota(jnp.int32, (experts, rows), 0) ^ me
    ids, wts = ids_ref[...], wts_ref[...]
    named = jnp.zeros((experts, rows), jnp.float32)
    weight = jnp.zeros((experts, rows), jnp.float32)
    for k in range(top):
        match = ids[k:k + 1] == expert_of
        named = named + jnp.where(match, 1.0, 0.0)
        weight = weight + jnp.where(match, wts[k:k + 1], 0.0)
    earlier = jnp.where(down < across, 1.0, 0.0).astype(jnp.bfloat16)
    rank = jnp.dot(named.astype(jnp.bfloat16), earlier, preferred_element_type=jnp.float32)
    rank = jnp.where(named > 0.5, rank, -1.0)
    meta[0:near] = rank[near:]
    meta[near:2 * near] = weight[near:]
    meta[2 * near:] = rank[:near]

    fetch.wait()
    values = x_ref[...].astype(jnp.float32)
    rows_normed = (
        values
        * lax.rsqrt(jnp.mean(values * values, axis=-1, keepdims=True) + 1e-06)
        * gain_ref[...]
    ).astype(jnp.bfloat16)
    for c in range(PIECES):
        normed[c] = rows_normed[:, c * part_w:(c + 1) * part_w]

    def pick_of(rank):
        count = rank.shape[0]
        slot = lax.broadcasted_iota(jnp.int32, (count, cap, rows), 1).astype(jnp.float32)
        taken = rank[:, None, :] == slot
        pick = jnp.where(taken, 1.0, 0.0).reshape(count * cap, rows).astype(jnp.bfloat16)
        return taken, pick

    def onehots(rank, weight):
        taken, pick = pick_of(rank)
        share = jnp.where(taken, weight[:, None, :], 0.0).reshape(near * cap, rows)
        high = share.astype(jnp.bfloat16)
        return pick, high, (share - high.astype(jnp.float32)).astype(jnp.bfloat16)

    pl.semaphore_wait(barrier, near + boundary)

    @pl.when(is_boundary)
    def _():
        meta_copy.start()
        for c in range(PIECES):
            dense[c].start()

    @pl.when(is_end)
    def _():
        emeta_copy.start()
        for c in range(PIECES):
            edense[c].start()

    pick, high, low = onehots(rank[:near], weight[:near])
    share_hi[...] = high
    share_lo[...] = low

    def dot(a, b):
        return jnp.dot(a, b, preferred_element_type=jnp.float32)

    half = tp_count * cap

    def pack_near(p):
        packed = dot(pick[p * half:(p + 1) * half], rows_normed)
        packed = packed.astype(jnp.bfloat16).reshape(tp_count, cap, width)
        for j in range(tp_count):
            if p or j:
                nsend[p * tp_count + j] = packed[j]
            else:
                nrecv[0] = packed[0]
        for j in range(tp_count):
            if p or j:
                near_out[p * tp_count + j].start()

    def hidden_of(gate_act, up_act):
        return (gate_act / (1.0 + jnp.exp(-gate_act)) * up_act).astype(jnp.bfloat16)

    def expert_near(p, waits):
        base = p * tp_count
        for g in waits:
            near_out[base + g].wait_recv()
        block = nrecv[base:base + tp_count].reshape(half, width)
        hidden = hidden_of(dot(block, wg[...]), dot(block, wu[...]))
        result = dot(hidden, wd[...]).astype(jnp.bfloat16).reshape(tp_count, cap, width)
        for j in range(tp_count):
            if p or j:
                nres[base + j] = result[j]
            else:
                nback[0] = result[0]

    def return_near(gs):
        for g in gs:
            near_ret[g].start()

    def forward_end(c):
        edense[c].wait_recv()
        forward[c].start()

    def end_meta():
        emeta_copy.wait_recv()
        meta_forward.start()
        epick[...] = pick_of(emeta[2 * near + tp_count:])[1]

    def pack_end():
        for c in range(PIECES):
            packed = dot(epick[...], eblock[c]).astype(jnp.bfloat16).reshape(tp_count, cap, part_w)
            nrecv[tp_count, :, c * part_w:(c + 1) * part_w] = packed[0]
            for j in range(1, tp_count):
                esend[j, :, c * part_w:(c + 1) * part_w] = packed[j]
        for j in range(1, tp_count):
            eout[j].start()

    def relay_meta(v):
        remote(meta.at[far_meta], rmeta.at[v], meta_s.at[0], meta_r.at[v],
               at(across_mid, 0)).wait_recv()
        ranks, weights = rmeta[v, 0:near], rmeta[v, near:]
        if v == 0:
            ranks = jnp.concatenate([ranks[tp_count:], ranks[:tp_count]], axis=0)
            weights = jnp.concatenate([weights[tp_count:], weights[:tp_count]], axis=0)
        rp, rh, rl = onehots(ranks, weights)
        rpick[v] = rp
        rshare_hi[v] = rh
        rshare_lo[v] = rl

    def relay_out(v, c):
        remote(normed.at[c], rblock.at[v, c], dense_s.at[c], dense_r.at[v, c],
               at(across_mid, 0)).wait_recv()
        packed = dot(rpick[v], rblock[v, c]).astype(jnp.bfloat16).reshape(near, cap, part_w)
        frecv[v, c, 0] = packed[0]
        for i in range(1, near):
            fsend[v, c, i] = packed[i]
        for i in list(range(tp_count, near)) + list(range(1, tp_count)):
            far_out[v, c, i].start()

    def far_in(v, c, waits):
        for j in waits:
            far_out[v, c, j].wait_recv()
        block = frecv[v, c].reshape(half, part_w)
        more_gate = dot(block, wg[c * part_w:(c + 1) * part_w])
        more_up = dot(block, wu[c * part_w:(c + 1) * part_w])
        gate_acc[...] = more_gate if c == 0 else gate_acc[...] + more_gate
        up_acc[...] = more_up if c == 0 else up_acc[...] + more_up

    def far_result(v, at_relay):
        hidden = hidden_of(gate_acc[...], up_acc[...])
        for c in range(PIECES):
            result = dot(hidden, wd[:, c * part_w:(c + 1) * part_w])
            result = result.astype(jnp.bfloat16).reshape(tp_count, cap, part_w)
            if at_relay:
                rback[v, c, 0] = result[0]
            for j in range(at_relay, tp_count):
                fres[v, c, j] = result[j]
            for j in range(at_relay, tp_count):
                far_ret[v, c, j].start()

    def combine(high, low, block):
        total = None
        for comb in (high, low):
            term = lax.dot_general(
                comb, block, (((0,), (0,)), ((), ())), preferred_element_type=jnp.float32
            )
            total = term if total is None else total + term
        return total

    def relay_back(v, c):
        for i in range(1, near):
            remote(fres.at[v, c, 0], rback.at[v, c, i], fret_s.at[v, c, 0],
                   fret_r.at[v, c, i], at(own_relay, 1)).wait_recv()
        block = rback[v, c].reshape(near * cap, part_w)
        rsend[v, c] = combine(rshare_hi[v], rshare_lo[v], block).astype(jnp.bfloat16)
        final[v, c].start()

    def combine_near():
        for g in range(1, near):
            near_ret[g].wait_recv()
        acc[...] = combine(share_hi[...], share_lo[...], nback[...].reshape(near * cap, width))

    def finish(c):
        final[0, c].wait_recv()
        part = acc[:, c * part_w:(c + 1) * part_w] + farback[c].astype(jnp.float32)
        out_ref[:, c * part_w:(c + 1) * part_w] = part.astype(out_ref.dtype)
        stores[c].start()

    others, everyone = range(1, tp_count), range(tp_count)
    second = range(tp_count, near)
    def weights_here():
        for load in loads:
            load.wait()

    @pl.when(is_boundary)
    def _():
        pack_near(0)
        pack_near(1)
        relay_meta(0)
        relay_out(0, 0)
        weights_here()
        expert_near(0, others)
        return_near(others)
        relay_out(0, 1)
        end_meta()
        forward_end(0)
        forward_end(1)
        relay_out(0, 2)
        forward_end(2)
        relay_out(0, 3)
        forward_end(3)
        pack_end()
        relay_meta(1)
        for c in range(3):
            far_in(0, c, others)
        relay_out(1, 0)
        far_in(0, 3, others)
        far_result(0, 1)
        relay_out(1, 1)
        expert_near(1, others)
        relay_out(1, 2)
        relay_back(0, 0)
        relay_back(0, 1)
        relay_out(1, 3)
        return_near(second)
        relay_back(0, 2)
        for c in range(PIECES):
            far_in(1, c, others)
        far_result(1, 1)
        relay_back(0, 3)
        for c in range(PIECES):
            relay_back(1, c)
        combine_near()
        for c in range(PIECES):
            finish(c)

    @pl.when(is_end)
    def _():
        pack_near(0)
        weights_here()
        expert_near(0, others)
        return_near(others)
        far_in(0, 0, everyone)
        expert_near(1, everyone)
        return_near(list(second)[:EARLY])
        for c in range(1, PIECES):
            far_in(0, c, everyone)
        far_result(0, 0)
        for c in range(PIECES):
            far_in(1, c, everyone)
        far_result(1, 0)
        return_near(list(second)[EARLY:])
        combine_near()
        for c in range(PIECES):
            finish(c)

    for store in stores:
        store.wait()
    for copy in dense + near_out[1:tp_count] + near_ret[1:]:
        copy.wait_send()
    for v in range(2):
        for c in range(PIECES):
            for j in range(1, tp_count):
                far_ret[v, c, j].wait_send()

    @pl.when(is_end)
    def _():
        emeta_copy.wait_send()
        for v in range(2):
            for c in range(PIECES):
                far_ret[v, c, 0].wait_send()

    @pl.when(is_boundary)
    def _():
        meta_copy.wait_send()
        meta_forward.wait_send()
        for copy in forward + near_out[tp_count:] + eout[1:]:
            copy.wait_send()
        for v in range(2):
            for c in range(PIECES):
                for i in range(1, near):
                    far_out[v, c, i].wait_send()
                final[v, c].wait_send()


def fused(ep_count, tp_count, tokens, norm_gain, route_ids, route_weights, w_gate, w_up, w_down):
    rows, width = tokens.shape
    hidden = w_gate.shape[2]
    experts = ep_count * tp_count
    near = 2 * tp_count
    cap = 3 * rows * route_ids.shape[1] // (2 * experts)
    part_w = width // PIECES
    vmem = pl.BlockSpec(memory_space=pltpu.VMEM)
    hbm = pl.BlockSpec(memory_space=pl.ANY)

    def b16(*shape):
        return pltpu.VMEM(shape, jnp.bfloat16)

    def f32(*shape):
        return pltpu.VMEM(shape, jnp.float32)

    def sems(*shape):
        return pltpu.SemaphoreType.DMA(shape)

    return pl.pallas_call(
        functools.partial(kernel, ep_count, tp_count, cap),
        out_shape=jax.ShapeDtypeStruct((rows, width), tokens.dtype),
        in_specs=[hbm] + [vmem] * 3 + [hbm] * 3,
        out_specs=hbm,
        scratch_shapes=[
            b16(rows, width), b16(rows, width), sems(1 + PIECES),
            b16(PIECES, rows, part_w), f32(3 * near, rows),
            b16(near * cap, rows), b16(near * cap, rows),
            *[b16(near, cap, width)] * 4,
            b16(PIECES, rows, part_w), f32(3 * near, rows),
            b16(tp_count * cap, rows), b16(tp_count, cap, width),
            b16(2, PIECES, rows, part_w), f32(2, 2 * near, rows),
            *[b16(2, near * cap, rows)] * 3,
            b16(2, PIECES, near, cap, part_w),
            b16(2, PIECES, tp_count, cap, part_w),
            b16(2, PIECES, tp_count, cap, part_w),
            b16(2, PIECES, near, cap, part_w),
            b16(2, PIECES, rows, part_w), b16(PIECES, rows, part_w),
            b16(width, hidden), b16(width, hidden), b16(hidden, width),
            f32(rows, width), f32(tp_count * cap, hidden), f32(tp_count * cap, hidden),
            sems(3), sems(PIECES), sems(PIECES), sems(PIECES), sems(2, PIECES),
            sems(2), sems(1), sems(2),
            sems(near), sems(near), sems(tp_count), sems(near), sems(near),
            sems(2, PIECES, near), sems(2, PIECES, tp_count),
            sems(2, PIECES, tp_count), sems(2, PIECES, near),
            sems(2, PIECES), sems(PIECES),
        ],
        compiler_params=pltpu.CompilerParams(
            collective_id=0, has_side_effects=True, vmem_limit_bytes=56 * 1024 * 1024
        ),
    )(tokens, norm_gain.reshape(1, width), route_ids.T, route_weights.T, w_gate, w_up, w_down)


def solution(mesh):
    ep_count, tp_count = mesh.shape["ep"], mesh.shape["tp"]

    def on_device(*args):
        rows, experts = args[0].shape[0], ep_count * tp_count
        cap = 3 * rows * args[2].shape[1] // (2 * experts)
        if ep_count != 4 or tp_count != 4 or cap % 8 or rows % 128 or args[0].shape[1] % 256:
            return plain(*args)
        return fused(ep_count, tp_count, *args)

    return jax.shard_map(
        on_device,
        mesh=mesh,
        in_specs=(
            P(("grp", "ep", "tp"), None),
            P(),
            P(("grp", "ep", "tp"), None),
            P(("grp", "ep", "tp"), None),
            P(("ep", "tp"), None, None),
            P(("ep", "tp"), None, None),
            P(("ep", "tp"), None, None),
        ),
        out_specs=P(("grp", "ep", "tp"), None),
        check_vma=False,
    )
```

```python
import functools

import jax
import jax.numpy as jnp
from jax import lax
from jax.experimental import pallas as pl
from jax.experimental.pallas import tpu as pltpu
from jax.sharding import PartitionSpec as P

MESH = pl.DeviceIdType.MESH


def plain(tokens, norm_gain, route_ids, route_weights, w_gate, w_up, w_down):
    tok_rows, model_width = tokens.shape
    top_count = route_ids.shape[1]
    ep_count = lax.axis_size("ep")
    tp_count = lax.axis_size("tp")
    experts = ep_count * tp_count
    capacity = 3 * tok_rows * top_count // (2 * experts)
    values = tokens.astype(jnp.float32)
    normed = (
        values * lax.rsqrt(jnp.mean(values * values, axis=-1, keepdims=True) + 1e-06) * norm_gain
    ).astype(jnp.bfloat16)
    flat_ids = route_ids.reshape(-1)
    onehot = (flat_ids[:, None] == jnp.arange(experts, dtype=jnp.int32)[None, :]).astype(jnp.int32)
    slot_index = jnp.sum((jnp.cumsum(onehot, axis=0) - onehot) * onehot, axis=-1)
    token_of = jnp.arange(tok_rows * top_count, dtype=jnp.int32) // top_count
    buffer = jnp.zeros((experts, capacity, model_width), jnp.bfloat16)
    buffer = buffer.at[flat_ids, slot_index].set(normed[token_of])
    received = lax.all_to_all(buffer, ("ep", "tp"), split_axis=0, concat_axis=0, tiled=True)
    flat_rows = received.reshape(-1, model_width)
    gate_act = jnp.dot(flat_rows, w_gate[0], preferred_element_type=jnp.float32)
    up_act = jnp.dot(flat_rows, w_up[0], preferred_element_type=jnp.float32)
    hidden = (jax.nn.silu(gate_act) * up_act).astype(jnp.bfloat16)
    result = jnp.dot(hidden, w_down[0], preferred_element_type=jnp.float32).astype(jnp.bfloat16)
    returned = lax.all_to_all(
        result.reshape(received.shape), ("ep", "tp"), split_axis=0, concat_axis=0, tiled=True
    )
    picked = (
        returned[flat_ids, slot_index].reshape(tok_rows, top_count, model_width).astype(jnp.float32)
    )
    return jnp.sum(picked * route_weights[:, :, None], axis=1).astype(jnp.bfloat16)


def flipped(index, bits):
    bit = 1
    while bit <= bits:
        if bits & bit:
            index = index + (1 - 2 * ((index // bit) % 2)) * bit
        bit *= 2
    return index


PIECES = 8
EARLY = 1
GROUPS = ((0, 1), (1, 3), (3, 8))


def kernel(
    ep_count, tp_count, cap,
    x_hbm, gain_hbm, ids_hbm, wts_hbm, wg_hbm, wu_hbm, wd_hbm, out_ref,
    x_ref, gain_ref, ids_ref, wts_ref, io_sem,
    normed, meta, share_hi, share_lo, nsend, nrecv, nres, nback,
    eblock, emeta, epick, esend,
    rblock, rmeta, rpick, rshare_hi, rshare_lo, fsend, frecv, fres, rback, rsend, farback,
    wg, wu, wd, acc, gate_acc, up_acc,
    w_sem, dense_s, fwd_s, edense_r, dense_r, meta_s, emeta_r, meta_r, near_s, near_r,
    eout_s, lend_r, nret_s, nret_r, far_s, far_r, fret_s, fret_r, final_s, final_r,
):
    ep, tp, grp = lax.axis_index("ep"), lax.axis_index("tp"), lax.axis_index("grp")
    rows, width = x_ref.shape
    part_w = width // PIECES
    top = ids_ref.shape[0]
    experts = ep_count * tp_count
    near = 2 * tp_count
    me = ep * tp_count + tp
    boundary = (ep + ep // 2) % 2
    place_of_me = (1 - boundary) * tp_count
    own_relay = 1 + ep // 2
    is_boundary, is_end = boundary == 1, boundary == 0

    def at(plane, j):
        return (grp, plane, flipped(tp, j))

    def remote(src, dst, s_sem, r_sem, target):
        return pltpu.make_async_remote_copy(
            src_ref=src, dst_ref=dst, send_sem=s_sem, recv_sem=r_sem,
            device_id=target, device_id_type=MESH,
        )

    barrier = pltpu.get_barrier_semaphore()

    def greet(target):
        pl.semaphore_signal(barrier, inc=1, device_id=target, device_id_type=MESH)

    greet(at(flipped(ep, 2), 0))

    @pl.when(is_boundary)
    def _():
        greet(at(flipped(ep, 3), 0))

    for g in range(near - 1, 0, -1):
        greet(at(flipped(ep, g // tp_count), g % tp_count))
    fetches = [
        pltpu.make_async_copy(src, dst, io_sem.at[i])
        for i, (src, dst) in enumerate((
            (x_hbm, x_ref), (gain_hbm, gain_ref), (ids_hbm, ids_ref), (wts_hbm, wts_ref)))
    ]
    for fetch in fetches:
        fetch.start()
    loads = [
        pltpu.make_async_copy(src.at[0], dst, w_sem.at[i])
        for i, (src, dst) in enumerate(((wg_hbm, wg), (wu_hbm, wu), (wd_hbm, wd)))
    ]
    partner, across_mid = flipped(ep, 1), flipped(ep, 3)
    planes = [ep, partner]
    dense = [
        remote(normed.at[c], rblock.at[0, c], dense_s, dense_r.at[0, c], at(across_mid, 0))
        for c in range(PIECES)
    ]
    forward = [
        remote(eblock.at[c], rblock.at[1, c], fwd_s, dense_r.at[1, c], at(across_mid, 0))
        for c in range(PIECES)
    ]
    edense = [
        remote(normed.at[c], eblock.at[c], dense_s, edense_r.at[c], at(partner, 0))
        for c in range(PIECES)
    ]
    far_meta = pl.ds(0, 2 * near)
    meta_copy = remote(meta.at[far_meta], rmeta.at[0], meta_s.at[0], meta_r.at[0],
                       at(across_mid, 0))
    meta_forward = remote(emeta.at[far_meta], rmeta.at[1], meta_s.at[1], meta_r.at[1],
                          at(across_mid, 0))
    emeta_copy = remote(meta, emeta, meta_s.at[0], emeta_r.at[0], at(partner, 0))
    near_out = [
        remote(nsend.at[g], nrecv.at[g], near_s, near_r.at[g // tp_count],
               at(planes[g // tp_count], g % tp_count))
        for g in range(near)
    ]
    side = tp_count // 2
    eout = [
        remote(esend.at[j], nrecv.at[tp_count + j], eout_s, near_r.at[1], at(ep, j))
        for j in range(side)
    ]
    lend = [
        remote(nsend.at[tp_count + side + k], esend.at[k], near_s, lend_r, at(ep, side))
        for k in range(side)
    ]
    pass_on = [
        remote(esend.at[k], nrecv.at[tp_count + side + k], eout_s, near_r.at[1], at(partner, k))
        for k in range(side)
    ]
    near_ret = [
        remote(nres.at[g], nback.at[g], nret_s, nret_r,
               at(planes[g // tp_count], g % tp_count))
        for g in range(near)
    ]
    far_out, far_ret, final = {}, {}, {}
    for v in range(2):
        for c in range(PIECES):
            for i in range(near):
                far_out[v, c, i] = remote(
                    fsend.at[v, c, i], frecv.at[v, c, i % tp_count], far_s,
                    far_r.at[v, c], at(planes[i // tp_count], i % tp_count))
            for j in range(tp_count):
                place = place_of_me + j
                far_ret[v, c, j] = remote(
                    fres.at[v, c, j], rback.at[v, c, place], fret_s, fret_r.at[v, c],
                    at(own_relay, j))
            final[v, c] = remote(rsend.at[v, c], farback.at[c], final_s, final_r.at[c],
                                 at(flipped(ep, 3 - v), 0))

    def drain(ref, sem):
        pltpu.make_async_copy(ref, ref, sem).wait()

    down = lax.broadcasted_iota(jnp.int32, (rows, rows), 0)
    across = lax.broadcasted_iota(jnp.int32, (rows, rows), 1)

    expert_of = lax.broadcasted_iota(jnp.int32, (experts, rows), 0) ^ me
    for fetch in fetches[2:]:
        fetch.wait()
    ids, wts = ids_ref[...], wts_ref[...]
    named = jnp.zeros((experts, rows), jnp.float32)
    weight = jnp.zeros((experts, rows), jnp.float32)
    for k in range(top):
        match = ids[k:k + 1] == expert_of
        named = named + jnp.where(match, 1.0, 0.0)
        weight = weight + jnp.where(match, wts[k:k + 1], 0.0)
    earlier = jnp.where(down < across, 1.0, 0.0).astype(jnp.bfloat16)
    rank = jnp.dot(named.astype(jnp.bfloat16), earlier, preferred_element_type=jnp.float32)
    rank = jnp.where(named > 0.5, rank, -1.0)
    meta[0:near] = rank[near:]
    meta[near:2 * near] = weight[near:]
    meta[2 * near:] = rank[:near]

    for fetch in fetches[:2]:
        fetch.wait()
    for load in loads:
        load.start()
    values = x_ref[...].astype(jnp.float32)
    rows_normed = (
        values
        * lax.rsqrt(jnp.mean(values * values, axis=-1, keepdims=True) + 1e-06)
        * gain_ref[...]
    ).astype(jnp.bfloat16)
    for c in range(PIECES):
        normed[c] = rows_normed[:, c * part_w:(c + 1) * part_w]

    def pick_of(rank):
        count = rank.shape[0]
        slot = lax.broadcasted_iota(jnp.int32, (count, cap, rows), 1).astype(jnp.float32)
        taken = rank[:, None, :] == slot
        pick = jnp.where(taken, 1.0, 0.0).reshape(count * cap, rows).astype(jnp.bfloat16)
        return taken, pick

    def onehots(rank, weight):
        taken, pick = pick_of(rank)
        share = jnp.where(taken, weight[:, None, :], 0.0).reshape(near * cap, rows)
        high = share.astype(jnp.bfloat16)
        return pick, high, (share - high.astype(jnp.float32)).astype(jnp.bfloat16)

    pl.semaphore_wait(barrier, near + boundary)

    @pl.when(is_boundary)
    def _():
        meta_copy.start()
        for c in range(PIECES):
            dense[c].start()

    @pl.when(is_end)
    def _():
        emeta_copy.start()
        for c in range(PIECES):
            edense[c].start()

    pick, high, low = onehots(rank[:near], weight[:near])
    share_hi[...] = high
    share_lo[...] = low

    def dot(a, b):
        return jnp.dot(a, b, preferred_element_type=jnp.float32)

    half = tp_count * cap

    def pack_near(p):
        packed = dot(pick[p * half:(p + 1) * half], rows_normed)
        packed = packed.astype(jnp.bfloat16).reshape(tp_count, cap, width)
        for j in range(tp_count):
            if p or j:
                nsend[p * tp_count + j] = packed[j]
            else:
                nrecv[0] = packed[0]
        send_near(range(2) if p else range(1, tp_count), p)

    def send_near(js, p=1):
        for j in js:
            near_out[p * tp_count + j].start()

    def hidden_of(gate_act, up_act):
        return (gate_act / (1.0 + jnp.exp(-gate_act)) * up_act).astype(jnp.bfloat16)

    def expert_near(p, first):
        base = p * tp_count
        drain(nrecv.at[pl.ds(base + first, tp_count - first)], near_r.at[p])
        block = nrecv[base:base + tp_count].reshape(half, width)
        hidden = hidden_of(dot(block, wg[...]), dot(block, wu[...]))
        result = dot(hidden, wd[...]).astype(jnp.bfloat16).reshape(tp_count, cap, width)
        for j in range(tp_count):
            if p or j:
                nres[base + j] = result[j]
            else:
                nback[0] = result[0]

    def return_near(gs):
        for g in gs:
            near_ret[g].start()

    def forward_end(c):
        edense[c].wait_recv()
        forward[c].start()

    def end_meta():
        emeta_copy.wait_recv()
        meta_forward.start()
        epick[...] = pick_of(emeta[2 * near + tp_count:2 * near + tp_count + side])[1]

    def pack_end():
        for c in range(PIECES):
            packed = dot(epick[...], eblock[c]).astype(jnp.bfloat16).reshape(side, cap, part_w)
            nrecv[tp_count, :, c * part_w:(c + 1) * part_w] = packed[0]
            for j in range(1, side):
                esend[j, :, c * part_w:(c + 1) * part_w] = packed[j]
        for j in range(1, side):
            eout[j].start()

    def pack_lend():
        packed = dot(pick[half + side * cap:], rows_normed)
        packed = packed.astype(jnp.bfloat16).reshape(tp_count - side, cap, width)
        for k in range(side):
            nsend[tp_count + side + k] = packed[k]
            lend[k].start()

    def send_lent():
        drain(esend, lend_r)
        for copy in pass_on:
            copy.start()

    def relay_meta(v):
        remote(meta.at[far_meta], rmeta.at[v], meta_s.at[0], meta_r.at[v],
               at(across_mid, 0)).wait_recv()
        ranks, weights = rmeta[v, 0:near], rmeta[v, near:]
        if v == 0:
            ranks = jnp.concatenate([ranks[tp_count:], ranks[:tp_count]], axis=0)
            weights = jnp.concatenate([weights[tp_count:], weights[:tp_count]], axis=0)
        rp, rh, rl = onehots(ranks, weights)
        rpick[v] = rp
        rshare_hi[v] = rh
        rshare_lo[v] = rl

    def relay_out(v, c):
        remote(normed.at[c], rblock.at[v, c], dense_s, dense_r.at[v, c],
               at(across_mid, 0)).wait_recv()
        packed = dot(rpick[v], rblock[v, c]).astype(jnp.bfloat16).reshape(near, cap, part_w)
        frecv[v, c, 0] = packed[0]
        for i in range(1, near):
            fsend[v, c, i] = packed[i]
        for i in list(range(tp_count, near)) + list(range(1, tp_count)):
            far_out[v, c, i].start()

    def far_in(v, c, first):
        drain(frecv.at[v, c, pl.ds(first, tp_count - first)], far_r.at[v, c])
        block = frecv[v, c].reshape(half, part_w)
        more_gate = dot(block, wg[c * part_w:(c + 1) * part_w])
        more_up = dot(block, wu[c * part_w:(c + 1) * part_w])
        gate_acc[...] = more_gate if c == 0 else gate_acc[...] + more_gate
        up_acc[...] = more_up if c == 0 else up_acc[...] + more_up

    def far_result(v, at_relay):
        hidden = hidden_of(gate_acc[...], up_acc[...])
        for lo, hi in GROUPS:
            result = dot(hidden, wd[:, lo * part_w:hi * part_w])
            result = result.astype(jnp.bfloat16).reshape(tp_count, cap, (hi - lo) * part_w)
            for c in range(lo, hi):
                part = result[:, :, (c - lo) * part_w:(c - lo + 1) * part_w]
                if at_relay:
                    rback[v, c, 0] = part[0]
                for j in range(at_relay, tp_count):
                    fres[v, c, j] = part[j]
                for j in range(at_relay, tp_count):
                    far_ret[v, c, j].start()

    def combine(high, low, block):
        total = None
        for comb in (high, low):
            term = lax.dot_general(
                comb, block, (((0,), (0,)), ((), ())), preferred_element_type=jnp.float32
            )
            total = term if total is None else total + term
        return total

    def relay_back(v, c):
        drain(rback.at[v, c, pl.ds(1, near - 1)], fret_r.at[v, c])
        block = rback[v, c].reshape(near * cap, part_w)
        rsend[v, c] = combine(rshare_hi[v], rshare_lo[v], block).astype(jnp.bfloat16)
        final[v, c].start()

    def combine_near():
        drain(nback.at[pl.ds(1, near - 1)], nret_r)
        acc[...] = combine(share_hi[...], share_lo[...], nback[...].reshape(near * cap, width))

    def finish(c):
        final[0, c].wait_recv()
        part = acc[:, c * part_w:(c + 1) * part_w] + farback[c].astype(jnp.float32)
        out_ref[:, c * part_w:(c + 1) * part_w] = part.astype(out_ref.dtype)

    others = range(1, tp_count)
    second = range(tp_count, near)

    def weights_here():
        for load in loads:
            load.wait()

    @pl.when(is_boundary)
    def _():
        pack_near(0)
        pack_near(1)
        relay_meta(0)
        last = PIECES - 1
        ahead = PIECES // 2
        for c in range(ahead):
            relay_out(0, c)
            if c == 0:
                weights_here()
                expert_near(0, 1)
                return_near(others)
        end_meta()
        for c in range(ahead - 1):
            forward_end(c)
        for c in range(ahead, PIECES):
            relay_out(0, c)
            forward_end(c - 1)
        forward_end(last)
        send_near(range(2, tp_count))
        pack_end()
        relay_meta(1)
        for c in range(PIECES // 2):
            far_in(0, c, 1)
        relay_out(1, 0)
        for c in range(PIECES // 2, PIECES):
            far_in(0, c, 1)
        far_result(0, 1)
        for c in range(1, PIECES - 1):
            relay_out(1, c)
        relay_back(0, 0)
        relay_out(1, last)
        relay_back(0, 1)
        expert_near(1, 1)
        return_near(second)
        relay_back(0, 2)
        relay_back(0, 3)
        for c in range(4, PIECES):
            far_in(1, 2 * c - 8, 1)
            far_in(1, 2 * c - 7, 1)
            relay_back(0, c)
        far_result(1, 1)
        for c in range(PIECES):
            relay_back(1, c)
        combine_near()
        for c in range(PIECES):
            finish(c)

    @pl.when(is_end)
    def _():
        pack_near(0)
        pack_lend()
        weights_here()
        expert_near(0, 1)
        return_near(others)
        send_lent()
        for c in range(PIECES):
            far_in(0, c, 0)
        far_result(0, 0)
        expert_near(1, 0)
        return_near(list(second)[:EARLY])
        for c in range(PIECES):
            far_in(1, c, 0)
        far_result(1, 0)
        return_near(list(second)[EARLY:])
        combine_near()
        for c in range(PIECES):
            finish(c)

    drain(normed, dense_s)
    drain(nres.at[pl.ds(1, near - 1)], nret_s)

    @pl.when(is_end)
    def _():
        drain(meta, meta_s.at[0])
        drain(nsend.at[pl.ds(1, tp_count + side - 1)], near_s)
        drain(esend, eout_s)
        drain(fres, fret_s)

    @pl.when(is_boundary)
    def _():
        drain(meta.at[far_meta], meta_s.at[0])
        drain(meta.at[far_meta], meta_s.at[1])
        drain(eblock, fwd_s)
        drain(nsend.at[pl.ds(1, near - 1)], near_s)
        drain(esend.at[pl.ds(1, side - 1)], eout_s)
        drain(fres.at[:, :, pl.ds(1, tp_count - 1)], fret_s)
        drain(fsend.at[:, :, pl.ds(1, near - 1)], far_s)
        drain(rsend, final_s)


def fused(ep_count, tp_count, tokens, norm_gain, route_ids, route_weights, w_gate, w_up, w_down):
    rows, width = tokens.shape
    hidden = w_gate.shape[2]
    experts = ep_count * tp_count
    near = 2 * tp_count
    cap = 3 * rows * route_ids.shape[1] // (2 * experts)
    part_w = width // PIECES
    vmem = pl.BlockSpec(memory_space=pltpu.VMEM)
    hbm = pl.BlockSpec(memory_space=pltpu.HBM)

    def b16(*shape):
        return pltpu.VMEM(shape, jnp.bfloat16)

    def f32(*shape):
        return pltpu.VMEM(shape, jnp.float32)

    def sems(*shape):
        return pltpu.SemaphoreType.DMA(shape)

    one = pltpu.SemaphoreType.DMA
    return pl.pallas_call(
        functools.partial(kernel, ep_count, tp_count, cap),
        out_shape=jax.ShapeDtypeStruct((rows, width), tokens.dtype),
        in_specs=[hbm] * 7,
        out_specs=vmem,
        scratch_shapes=[
            b16(rows, width), f32(1, width),
            pltpu.VMEM(route_ids.shape[::-1], jnp.int32), f32(*route_weights.shape[::-1]), sems(4),
            b16(PIECES, rows, part_w), f32(3 * near, rows),
            b16(near * cap, rows), b16(near * cap, rows),
            *[b16(near, cap, width)] * 4,
            b16(PIECES, rows, part_w), f32(3 * near, rows),
            b16(tp_count // 2 * cap, rows), b16(tp_count // 2, cap, width),
            b16(2, PIECES, rows, part_w), f32(2, 2 * near, rows),
            *[b16(2, near * cap, rows)] * 3,
            b16(2, PIECES, near, cap, part_w),
            b16(2, PIECES, tp_count, cap, part_w),
            b16(2, PIECES, tp_count, cap, part_w),
            b16(2, PIECES, near, cap, part_w),
            b16(2, PIECES, rows, part_w), b16(PIECES, rows, part_w),
            b16(width, hidden), b16(width, hidden), b16(hidden, width),
            f32(rows, width), f32(tp_count * cap, hidden), f32(tp_count * cap, hidden),
            sems(3), one, one, sems(PIECES), sems(2, PIECES),
            sems(2), sems(1), sems(2), one, sems(2), one, one, one, one,
            one, sems(2, PIECES), one, sems(2, PIECES), one, sems(PIECES),
        ],
        compiler_params=pltpu.CompilerParams(
            collective_id=0, has_side_effects=True, vmem_limit_bytes=32 * 1024 * 1024
        ),
    )(*(
        pltpu.with_memory_space_constraint(arg, pltpu.HBM)
        for arg in (tokens, norm_gain.reshape(1, width), route_ids.T, route_weights.T,
                    w_gate, w_up, w_down)
    ))


def solution(mesh):
    ep_count, tp_count = mesh.shape["ep"], mesh.shape["tp"]

    def on_device(*args):
        rows, experts = args[0].shape[0], ep_count * tp_count
        cap = 3 * rows * args[2].shape[1] // (2 * experts)
        if ep_count != 4 or tp_count != 4 or cap % 8 or rows % 128 or args[0].shape[1] % 256:
            return plain(*args)
        return fused(ep_count, tp_count, *args)

    return jax.shard_map(
        on_device,
        mesh=mesh,
        in_specs=(
            P(("grp", "ep", "tp"), None),
            P(),
            P(("grp", "ep", "tp"), None),
            P(("grp", "ep", "tp"), None),
            P(("ep", "tp"), None, None),
            P(("ep", "tp"), None, None),
            P(("ep", "tp"), None, None),
        ),
        out_specs=P(("grp", "ep", "tp"), None),
        check_vma=False,
    )
```

```python
import functools

import jax
import jax.numpy as jnp
from jax import lax
from jax.experimental import pallas as pl
from jax.experimental.pallas import tpu as pltpu
from jax.sharding import PartitionSpec as P

MESH = pl.DeviceIdType.MESH


def plain(tokens, norm_gain, route_ids, route_weights, w_gate, w_up, w_down):
    tok_rows, model_width = tokens.shape
    top_count = route_ids.shape[1]
    ep_count = lax.axis_size("ep")
    tp_count = lax.axis_size("tp")
    experts = ep_count * tp_count
    capacity = 3 * tok_rows * top_count // (2 * experts)
    values = tokens.astype(jnp.float32)
    normed = (
        values * lax.rsqrt(jnp.mean(values * values, axis=-1, keepdims=True) + 1e-06) * norm_gain
    ).astype(jnp.bfloat16)
    flat_ids = route_ids.reshape(-1)
    onehot = (flat_ids[:, None] == jnp.arange(experts, dtype=jnp.int32)[None, :]).astype(jnp.int32)
    slot_index = jnp.sum((jnp.cumsum(onehot, axis=0) - onehot) * onehot, axis=-1)
    token_of = jnp.arange(tok_rows * top_count, dtype=jnp.int32) // top_count
    buffer = jnp.zeros((experts, capacity, model_width), jnp.bfloat16)
    buffer = buffer.at[flat_ids, slot_index].set(normed[token_of])
    received = lax.all_to_all(buffer, ("ep", "tp"), split_axis=0, concat_axis=0, tiled=True)
    flat_rows = received.reshape(-1, model_width)
    gate_act = jnp.dot(flat_rows, w_gate[0], preferred_element_type=jnp.float32)
    up_act = jnp.dot(flat_rows, w_up[0], preferred_element_type=jnp.float32)
    hidden = (jax.nn.silu(gate_act) * up_act).astype(jnp.bfloat16)
    result = jnp.dot(hidden, w_down[0], preferred_element_type=jnp.float32).astype(jnp.bfloat16)
    returned = lax.all_to_all(
        result.reshape(received.shape), ("ep", "tp"), split_axis=0, concat_axis=0, tiled=True
    )
    picked = (
        returned[flat_ids, slot_index].reshape(tok_rows, top_count, model_width).astype(jnp.float32)
    )
    return jnp.sum(picked * route_weights[:, :, None], axis=1).astype(jnp.bfloat16)


def flipped(index, bits):
    bit = 1
    while bit <= bits:
        if bits & bit:
            index = index + (1 - 2 * ((index // bit) % 2)) * bit
        bit *= 2
    return index


PIECES = 8
EARLY = 1
AHEAD = 3
DIRECT = 2
GROUPS = ((0, 1), (1, 3), (3, 8))
DENSE_BY = (0, 2, 4, 6, 7, 8)
EDENSE_BY = (0, 2, 4, 6, 8)
FAR_BY = (0, 4, 6, 7, 8)
BACK_BY = (0, 1, 2, 3, 4, 5, 6, 7, 8)
HOP_BY = (DIRECT, 4, 6, 8)
FINAL_BY = (0, 6, 7, 8)


def span(edges, c):
    g = max(i for i in range(len(edges) - 1) if edges[i] <= c)
    return g, edges[g], edges[g + 1] - edges[g]


def slot(edges, c):
    return span(edges, c)[0]


def kernel(
    ep_count, tp_count, cap,
    x_hbm, gain_hbm, ids_hbm, wts_hbm, wg_hbm, wu_hbm, wd_hbm, out_ref,
    x_ref, gain_ref, ids_ref, wts_ref, io_sem,
    normed, meta, share_hi, share_lo, nsend, nrecv, nres, nback,
    eblock, emeta, epick, esend, hop,
    rblock, rmeta, rpick, rshare_hi, rshare_lo, fsend, frecv, fres, rback, rsend, farback,
    wg, wu, wd, acc, gate_acc, up_acc,
    w_sem, ready, dense_s, fwd_s, edense_r, dense_r, meta_s, emeta_r, meta_r, near_s, near_r,
    eout_s, lend_r, nret_s, nret_r, far_s, far_r, fret_s, fret_r, hop_s, hop_r, final_s, final_r,
):
    ep, tp, grp = lax.axis_index("ep"), lax.axis_index("tp"), lax.axis_index("grp")
    rows, width = x_ref.shape
    part_w = width // PIECES
    top = ids_ref.shape[0]
    experts = ep_count * tp_count
    near = 2 * tp_count
    me = ep * tp_count + tp
    boundary = (ep + ep // 2) % 2
    place_of_me = (1 - boundary) * tp_count
    own_relay = 1 + ep // 2
    is_boundary, is_end = boundary == 1, boundary == 0
    is_first = ep < ep_count // 2
    holds_back = jnp.logical_and(ep == ep_count // 2, tp % 2 == 0)

    def at(plane, j):
        return (grp, plane, flipped(tp, j))

    def remote(src, dst, s_sem, r_sem, target):
        return pltpu.make_async_remote_copy(
            src_ref=src, dst_ref=dst, send_sem=s_sem, recv_sem=r_sem,
            device_id=target, device_id_type=MESH,
        )

    barrier = pltpu.get_barrier_semaphore()

    def greet(target):
        pl.semaphore_signal(barrier, inc=1, device_id=target, device_id_type=MESH)

    @pl.when(is_boundary)
    def _():
        greet(at(flipped(ep, 3), 0))
        for j in range(tp_count):
            greet(at(flipped(ep, 1), j))

    @pl.when(jnp.logical_and(is_end, is_first))
    def _():
        for j in range(tp_count):
            greet(at(flipped(ep, 1), j))

    for j in range(1, tp_count):
        greet(at(ep, j))
    fetches = [
        pltpu.make_async_copy(src, dst, io_sem.at[i])
        for i, (src, dst) in enumerate((
            (x_hbm, x_ref), (gain_hbm, gain_ref), (ids_hbm, ids_ref), (wts_hbm, wts_ref)))
    ]
    for fetch in fetches:
        fetch.start()
    loads = [
        pltpu.make_async_copy(src.at[0], dst, w_sem.at[i])
        for i, (src, dst) in enumerate(((wg_hbm, wg), (wu_hbm, wu), (wd_hbm, wd)))
    ]
    partner, across_mid = flipped(ep, 1), flipped(ep, 3)

    @pl.when(is_end)
    def _():
        pl.semaphore_wait(barrier, near - 1)

    @pl.when(jnp.logical_and(is_end, jnp.logical_not(is_first)))
    def _():
        for j in range(tp_count):
            pl.semaphore_signal(ready, inc=1, device_id=at(partner, j), device_id_type=MESH)

    planes = [ep, partner]
    dense = [
        remote(normed.at[c], rblock.at[0, c], dense_s, dense_r.at[0, slot(DENSE_BY, c)], at(across_mid, 0))
        for c in range(PIECES)
    ]
    forward = [
        remote(eblock.at[c], rblock.at[1, c], fwd_s, dense_r.at[1, slot(DENSE_BY, c)], at(across_mid, 0))
        for c in range(PIECES)
    ]
    edense = [
        remote(normed.at[c], eblock.at[c], dense_s, edense_r.at[slot(EDENSE_BY, c)], at(partner, 0))
        for c in range(PIECES)
    ]
    far_meta = pl.ds(0, 2 * near)
    meta_copy = remote(meta.at[far_meta], rmeta.at[0], meta_s.at[0], meta_r.at[0],
                       at(across_mid, 0))
    meta_forward = remote(emeta.at[far_meta], rmeta.at[1], meta_s.at[1], meta_r.at[1],
                          at(across_mid, 0))
    emeta_copy = remote(meta, emeta, meta_s.at[0], emeta_r.at[0], at(partner, 0))
    near_out = [
        remote(nsend.at[g], nrecv.at[g], near_s, near_r.at[max(0, 2 * g // tp_count - 1)],
               at(planes[g // tp_count], g % tp_count))
        for g in range(near)
    ]
    side = tp_count // 2
    eout = [
        remote(esend.at[j], nrecv.at[tp_count + j], eout_s, near_r.at[1], at(ep, j))
        for j in range(side)
    ]
    lend = [
        remote(nsend.at[tp_count + side + k], esend.at[k], near_s, lend_r, at(ep, side))
        for k in range(side)
    ]
    pass_on = [
        remote(esend.at[k], nrecv.at[tp_count + side + k], eout_s, near_r.at[1], at(partner, k))
        for k in range(side)
    ]
    near_ret = [
        remote(nres.at[g], nback.at[g], nret_s, nret_r,
               at(planes[g // tp_count], g % tp_count))
        for g in range(near)
    ]
    far_out, far_ret, to_hop, from_hop, final = {}, {}, {}, {}, {}
    for v in range(2):
        for c in range(PIECES):
            for i in range(near):
                far_out[v, c, i] = remote(
                    fsend.at[v, c, i], frecv.at[v, c, i % tp_count], far_s,
                    far_r.at[v, slot(FAR_BY, c)], at(planes[i // tp_count], i % tp_count))
            for j in range(tp_count):
                place = place_of_me + j
                far_ret[v, c, j] = remote(
                    fres.at[v, c, j], rback.at[v, c, place], fret_s, fret_r.at[v, slot(BACK_BY, c)],
                    at(own_relay, j))
            if v == 0 and c >= DIRECT:
                for j in range(side, tp_count):
                    to_hop[c, j] = remote(fres.at[v, c, j], hop.at[c, j - side], fret_s,
                                          hop_r.at[slot(HOP_BY, c)], at(ep, j))
                from_hop[c] = remote(hop.at[c], rback.at[v, c, pl.ds(tp_count + side, side)],
                                     hop_s, fret_r.at[v, slot(BACK_BY, c)], at(own_relay, 0))
            final[v, c] = remote(rsend.at[v, c], farback.at[c], final_s, final_r.at[slot(FINAL_BY, c)],
                                 at(flipped(ep, 3 - v), 0))

    def drain(ref, sem):
        pltpu.make_async_copy(ref, ref, sem).wait()

    down = lax.broadcasted_iota(jnp.int32, (rows, rows), 0)
    across = lax.broadcasted_iota(jnp.int32, (rows, rows), 1)

    expert_of = lax.broadcasted_iota(jnp.int32, (experts, rows), 0) ^ me
    for fetch in fetches[2:]:
        fetch.wait()
    ids, wts = ids_ref[...], wts_ref[...]
    named = jnp.zeros((experts, rows), jnp.float32)
    weight = jnp.zeros((experts, rows), jnp.float32)
    for k in range(top):
        match = ids[k:k + 1] == expert_of
        named = named + jnp.where(match, 1.0, 0.0)
        weight = weight + jnp.where(match, wts[k:k + 1], 0.0)
    earlier = jnp.where(down < across, 1.0, 0.0).astype(jnp.bfloat16)
    rank = jnp.dot(named.astype(jnp.bfloat16), earlier, preferred_element_type=jnp.float32)
    rank = jnp.where(named > 0.5, rank, -1.0)
    meta[0:near] = rank[near:]
    meta[near:2 * near] = weight[near:]
    meta[2 * near:] = rank[:near]

    for fetch in fetches[:2]:
        fetch.wait()
    for load in loads:
        load.start()
    values = x_ref[...].astype(jnp.float32)
    rows_normed = (
        values
        * lax.rsqrt(jnp.mean(values * values, axis=-1, keepdims=True) + 1e-06)
        * gain_ref[...]
    ).astype(jnp.bfloat16)
    for c in range(PIECES):
        normed[c] = rows_normed[:, c * part_w:(c + 1) * part_w]

    @pl.when(is_boundary)
    def _():
        pl.semaphore_wait(barrier, tp_count + jnp.where(is_first, tp_count, 0))
        meta_copy.start()
        for c in range(PIECES):
            dense[c].start()

    @pl.when(is_end)
    def _():
        emeta_copy.start()
        for c in range(PIECES):
            edense[c].start()

    def pick_of(rank):
        count = rank.shape[0]
        slot = lax.broadcasted_iota(jnp.int32, (count, cap, rows), 1).astype(jnp.float32)
        taken = rank[:, None, :] == slot
        pick = jnp.where(taken, 1.0, 0.0).reshape(count * cap, rows).astype(jnp.bfloat16)
        return taken, pick

    def onehots(rank, weight):
        taken, pick = pick_of(rank)
        share = jnp.where(taken, weight[:, None, :], 0.0).reshape(near * cap, rows)
        high = share.astype(jnp.bfloat16)
        return pick, high, (share - high.astype(jnp.float32)).astype(jnp.bfloat16)

    pick, high, low = onehots(rank[:near], weight[:near])

    def dot(a, b):
        return jnp.dot(a, b, preferred_element_type=jnp.float32)

    half = tp_count * cap
    crossing = [*range(side, tp_count), *range(side - 1, -1, -1)]

    def pack_near(p):
        packed = dot(pick[p * half:(p + 1) * half], rows_normed)
        packed = packed.astype(jnp.bfloat16).reshape(tp_count, cap, width)
        for j in range(tp_count):
            if p or j:
                nsend[p * tp_count + j] = packed[j]
            else:
                nrecv[0] = packed[0]

    pack_near(1)

    share_hi[...] = high
    share_lo[...] = low

    def send_near(js, p=1):
        for j in js:
            near_out[p * tp_count + j].start()

    def hidden_of(gate_act, up_act):
        return (gate_act / (1.0 + jnp.exp(-gate_act)) * up_act).astype(jnp.bfloat16)

    def near_part(base, first, count, sem):
        drain(nrecv.at[pl.ds(base + first, count - first)], near_r.at[sem])
        block = nrecv[base:base + count].reshape(count * cap, width)
        hidden = hidden_of(dot(block, wg[...]), dot(block, wu[...]))
        result = dot(hidden, wd[...]).astype(jnp.bfloat16).reshape(count, cap, width)
        for j in range(count):
            if base or j:
                nres[base + j] = result[j]
            else:
                nback[0] = result[0]

    def expert_near(p, first):
        near_part(p * tp_count, first, tp_count, p)

    def return_near(gs):
        for g in gs:
            near_ret[g].start()

    def forward_end(c):
        g, lo, count = span(EDENSE_BY, c)
        if c == lo:
            drain(eblock.at[pl.ds(lo, count)], edense_r.at[g])
        forward[c].start()

    def end_meta():
        emeta_copy.wait_recv()
        meta_forward.start()
        epick[...] = pick_of(emeta[2 * near + tp_count:2 * near + tp_count + side])[1]

    def pack_end():
        for c in range(PIECES):
            packed = dot(epick[...], eblock[c]).astype(jnp.bfloat16).reshape(side, cap, part_w)
            nrecv[tp_count, :, c * part_w:(c + 1) * part_w] = packed[0]
            for j in range(1, side):
                esend[j, :, c * part_w:(c + 1) * part_w] = packed[j]
        for j in range(1, side):
            eout[j].start()

    def send_lend():
        for copy in lend:
            copy.start()

    def send_lent():
        drain(esend, lend_r)
        for copy in pass_on:
            copy.start()

    def relay_meta(v):
        remote(meta.at[far_meta], rmeta.at[v], meta_s.at[0], meta_r.at[v],
               at(across_mid, 0)).wait_recv()
        ranks, weights = rmeta[v, 0:near], rmeta[v, near:]
        if v == 0:
            ranks = jnp.concatenate([ranks[tp_count:], ranks[:tp_count]], axis=0)
            weights = jnp.concatenate([weights[tp_count:], weights[:tp_count]], axis=0)
        rp, rh, rl = onehots(ranks, weights)
        rpick[v] = rp
        rshare_hi[v] = rh
        rshare_lo[v] = rl

    def relay_out(v, c):
        g, lo, count = span(DENSE_BY, c)
        if c == lo:
            drain(rblock.at[v, pl.ds(lo, count)], dense_r.at[v, g])
        packed = dot(rpick[v], rblock[v, c]).astype(jnp.bfloat16).reshape(near, cap, part_w)
        frecv[v, c, 0] = packed[0]
        for i in range(1, near):
            fsend[v, c, i] = packed[i]
        for i in list(range(tp_count + side, near)) + list(range(tp_count, tp_count + side)) + crossing[:-1]:
            far_out[v, c, i].start()

    def far_in(v, c, first):
        g, lo, count = span(FAR_BY, c)
        if c == lo:
            drain(frecv.at[v, pl.ds(lo, count), pl.ds(first, tp_count - first)], far_r.at[v, g])
        block = frecv[v, c].reshape(half, part_w)
        more_gate = dot(block, wg[c * part_w:(c + 1) * part_w])
        more_up = dot(block, wu[c * part_w:(c + 1) * part_w])
        gate_acc[...] = more_gate if c == 0 else gate_acc[...] + more_gate
        up_acc[...] = more_up if c == 0 else up_acc[...] + more_up

    def far_result(v, at_relay):
        hidden = hidden_of(gate_acc[...], up_acc[...])
        for lo, hi in GROUPS:
            result = dot(hidden, wd[:, lo * part_w:hi * part_w])
            result = result.astype(jnp.bfloat16).reshape(tp_count, cap, (hi - lo) * part_w)
            for c in range(lo, hi):
                part = result[:, :, (c - lo) * part_w:(c - lo + 1) * part_w]
                if at_relay:
                    rback[v, c, 0] = part[0]
                for j in range(at_relay, tp_count):
                    fres[v, c, j] = part[j]
                for j in crossing[:tp_count - at_relay]:
                    if not at_relay and (c, j) in to_hop and v == 0:
                        to_hop[c, j].start()
                    else:
                        far_ret[v, c, j].start()

    def hop_on(c):
        g, lo, count = span(HOP_BY, c)
        if c == lo:
            drain(hop.at[pl.ds(lo, count)], hop_r.at[g])
        from_hop[c].start()

    def combine(high, low, block):
        total = None
        for comb in (high, low):
            term = lax.dot_general(
                comb, block, (((0,), (0,)), ((), ())), preferred_element_type=jnp.float32
            )
            total = term if total is None else total + term
        return total

    def relay_back(v, c):
        g, lo, count = span(BACK_BY, c)
        if c == lo:
            drain(rback.at[v, pl.ds(lo, count), pl.ds(1, near - 1)], fret_r.at[v, g])
        block = rback[v, c].reshape(near * cap, part_w)
        rsend[v, c] = combine(rshare_hi[v], rshare_lo[v], block).astype(jnp.bfloat16)
        final[v, c].start()

    def combine_near():
        drain(nback.at[pl.ds(1, near - 1)], nret_r)
        acc[...] = combine(share_hi[...], share_lo[...], nback[...].reshape(near * cap, width))

    def finish(c):
        g, lo, count = span(FINAL_BY, c)
        if c == lo:
            drain(farback.at[pl.ds(lo, count)], final_r.at[g])
        part = acc[:, c * part_w:(c + 1) * part_w] + farback[c].astype(jnp.float32)
        out_ref[:, c * part_w:(c + 1) * part_w] = part.astype(out_ref.dtype)

    others = range(1, tp_count)
    second = range(tp_count, near)

    def ends_here():
        @pl.when(jnp.logical_not(is_first))
        def _():
            pl.semaphore_wait(ready, tp_count)

    def weights_here():
        for load in loads:
            load.wait()

    @pl.when(is_boundary)
    def _():
        @pl.when(is_first)
        def _():
            send_near(range(AHEAD))

        pack_near(0)
        send_near(range(1, tp_count), 0)
        ends_here()

        @pl.when(jnp.logical_not(is_first))
        def _():
            send_near(range(AHEAD))

        relay_meta(0)
        last = PIECES - 1
        ahead = PIECES // 2
        for c in range(ahead):
            relay_out(0, c)
            if c == 0:
                weights_here()
                expert_near(0, 1)
                return_near(others)
        end_meta()
        for c in range(ahead - 1):
            forward_end(c)
        for c in range(ahead, PIECES):
            relay_out(0, c)
            forward_end(c - 1)
        forward_end(last)
        send_near(range(AHEAD, tp_count))
        pack_end()
        relay_meta(1)
        for c in range(PIECES // 2):
            far_in(0, c, 1)
        relay_out(1, 0)
        for c in range(PIECES // 2, PIECES):
            far_in(0, c, 1)
        far_result(0, 1)
        relay_out(1, 1)
        expert_near(1, 1)
        for c in range(2, PIECES - 3):
            relay_out(1, c)
        relay_back(0, 0)
        relay_out(1, last - 2)
        relay_back(0, 1)
        relay_out(1, last - 1)
        relay_out(1, last)

        @pl.when(tp < side)
        def _():
            return_near(second)

        @pl.when(tp >= side)
        def _():
            return_near(second[::-1])

        relay_back(0, 2)
        relay_back(0, 3)
        for c in range(4, 6):
            far_in(1, 2 * c - 8, 1)
            far_in(1, 2 * c - 7, 1)
            relay_back(0, c)
        for c in range(4, PIECES):
            far_in(1, c, 1)
        far_result(1, 1)
        relay_back(0, last - 1)

        @pl.when(jnp.logical_not(holds_back))
        def _():
            relay_back(0, last)

        for c in range(PIECES):
            relay_back(1, c)

        @pl.when(holds_back)
        def _():
            relay_back(0, last)

        combine_near()
        for c in range(PIECES):
            finish(c)

    @pl.when(is_end)
    def _():
        send_lend()
        pack_near(0)
        send_near(range(1, tp_count), 0)
        send_lent()
        weights_here()
        near_part(tp_count, 0, side, 1)
        return_near(list(second)[:EARLY])
        for c in range(PIECES):
            far_in(0, c, 0)
        far_result(0, 0)
        for c in range(DIRECT, PIECES):
            if c == DIRECT + 2:
                expert_near(0, 1)
            if c == DIRECT + 4:
                near_part(tp_count + side, 0, tp_count - side, 2)
            hop_on(c)
        for c in range(PIECES):
            far_in(1, c, 0)
        far_result(1, 0)
        return_near(others)
        return_near(list(second)[EARLY:])
        combine_near()
        for c in range(PIECES):
            finish(c)

    drain(normed, dense_s)
    drain(nres.at[pl.ds(1, near - 1)], nret_s)

    @pl.when(is_end)
    def _():
        drain(meta, meta_s.at[0])
        drain(nsend.at[pl.ds(1, tp_count + side - 1)], near_s)
        drain(esend, eout_s)
        drain(fres, fret_s)
        drain(hop.at[pl.ds(DIRECT, PIECES - DIRECT)], hop_s)

    @pl.when(is_boundary)
    def _():
        drain(meta.at[far_meta], meta_s.at[0])
        drain(meta.at[far_meta], meta_s.at[1])
        drain(eblock, fwd_s)
        drain(nsend.at[pl.ds(1, near - 1)], near_s)
        drain(esend.at[pl.ds(1, side - 1)], eout_s)
        drain(fres.at[:, :, pl.ds(1, tp_count - 1)], fret_s)
        drain(fsend.at[:, :, pl.ds(1, near - 1)], far_s)
        drain(rsend, final_s)


def fused(ep_count, tp_count, tokens, norm_gain, route_ids, route_weights, w_gate, w_up, w_down):
    rows, width = tokens.shape
    hidden = w_gate.shape[2]
    experts = ep_count * tp_count
    near = 2 * tp_count
    cap = 3 * rows * route_ids.shape[1] // (2 * experts)
    part_w = width // PIECES
    vmem = pl.BlockSpec(memory_space=pltpu.VMEM)
    hbm = pl.BlockSpec(memory_space=pltpu.HBM)

    def b16(*shape):
        return pltpu.VMEM(shape, jnp.bfloat16)

    def f32(*shape):
        return pltpu.VMEM(shape, jnp.float32)

    def sems(*shape):
        return pltpu.SemaphoreType.DMA(shape)

    one = pltpu.SemaphoreType.DMA
    return pl.pallas_call(
        functools.partial(kernel, ep_count, tp_count, cap),
        out_shape=jax.ShapeDtypeStruct((rows, width), tokens.dtype),
        in_specs=[hbm] * 7,
        out_specs=vmem,
        scratch_shapes=[
            b16(rows, width), f32(1, width),
            pltpu.VMEM(route_ids.shape[::-1], jnp.int32), f32(*route_weights.shape[::-1]), sems(4),
            b16(PIECES, rows, part_w), f32(3 * near, rows),
            b16(near * cap, rows), b16(near * cap, rows),
            *[b16(near, cap, width)] * 4,
            b16(PIECES, rows, part_w), f32(3 * near, rows),
            b16(tp_count // 2 * cap, rows), b16(tp_count // 2, cap, width),
            b16(PIECES, tp_count // 2, cap, part_w),
            b16(2, PIECES, rows, part_w), f32(2, 2 * near, rows),
            *[b16(2, near * cap, rows)] * 3,
            b16(2, PIECES, near, cap, part_w),
            b16(2, PIECES, tp_count, cap, part_w),
            b16(2, PIECES, tp_count, cap, part_w),
            b16(2, PIECES, near, cap, part_w),
            b16(2, PIECES, rows, part_w), b16(PIECES, rows, part_w),
            b16(width, hidden), b16(width, hidden), b16(hidden, width),
            f32(rows, width), f32(tp_count * cap, hidden), f32(tp_count * cap, hidden),
            sems(3), pltpu.SemaphoreType.REGULAR, one, one,
            sems(len(EDENSE_BY) - 1), sems(2, len(DENSE_BY) - 1),
            sems(2), sems(1), sems(2), one, sems(3), one, one, one, one,
            one, sems(2, len(FAR_BY) - 1), one, sems(2, len(BACK_BY) - 1),
            one, sems(len(HOP_BY) - 1), one, sems(len(FINAL_BY) - 1),
        ],
        compiler_params=pltpu.CompilerParams(
            collective_id=0, has_side_effects=True, vmem_limit_bytes=32 * 1024 * 1024
        ),
    )(*(
        pltpu.with_memory_space_constraint(arg, pltpu.HBM)
        for arg in (tokens, norm_gain.reshape(1, width), route_ids.T, route_weights.T,
                    w_gate, w_up, w_down)
    ))


def solution(mesh):
    ep_count, tp_count = mesh.shape["ep"], mesh.shape["tp"]

    def on_device(*args):
        rows, experts = args[0].shape[0], ep_count * tp_count
        cap = 3 * rows * args[2].shape[1] // (2 * experts)
        if ep_count != 4 or tp_count != 4 or cap % 8 or rows % 128 or args[0].shape[1] % 256:
            return plain(*args)
        return fused(ep_count, tp_count, *args)

    return jax.shard_map(
        on_device,
        mesh=mesh,
        in_specs=(
            P(("grp", "ep", "tp"), None),
            P(),
            P(("grp", "ep", "tp"), None),
            P(("grp", "ep", "tp"), None),
            P(("ep", "tp"), None, None),
            P(("ep", "tp"), None, None),
            P(("ep", "tp"), None, None),
        ),
        out_specs=P(("grp", "ep", "tp"), None),
        check_vma=False,
    )
```

```python
import functools

import jax
import jax.numpy as jnp
from jax import lax
from jax.experimental import pallas as pl
from jax.experimental.pallas import tpu as pltpu
from jax.sharding import PartitionSpec as P

MESH = pl.DeviceIdType.MESH


def plain(tokens, norm_gain, route_ids, route_weights, w_gate, w_up, w_down):
    tok_rows, model_width = tokens.shape
    top_count = route_ids.shape[1]
    ep_count = lax.axis_size("ep")
    tp_count = lax.axis_size("tp")
    experts = ep_count * tp_count
    capacity = 3 * tok_rows * top_count // (2 * experts)
    values = tokens.astype(jnp.float32)
    normed = (
        values * lax.rsqrt(jnp.mean(values * values, axis=-1, keepdims=True) + 1e-06) * norm_gain
    ).astype(jnp.bfloat16)
    flat_ids = route_ids.reshape(-1)
    onehot = (flat_ids[:, None] == jnp.arange(experts, dtype=jnp.int32)[None, :]).astype(jnp.int32)
    slot_index = jnp.sum((jnp.cumsum(onehot, axis=0) - onehot) * onehot, axis=-1)
    token_of = jnp.arange(tok_rows * top_count, dtype=jnp.int32) // top_count
    buffer = jnp.zeros((experts, capacity, model_width), jnp.bfloat16)
    buffer = buffer.at[flat_ids, slot_index].set(normed[token_of])
    received = lax.all_to_all(buffer, ("ep", "tp"), split_axis=0, concat_axis=0, tiled=True)
    flat_rows = received.reshape(-1, model_width)
    gate_act = jnp.dot(flat_rows, w_gate[0], preferred_element_type=jnp.float32)
    up_act = jnp.dot(flat_rows, w_up[0], preferred_element_type=jnp.float32)
    hidden = (jax.nn.silu(gate_act) * up_act).astype(jnp.bfloat16)
    result = jnp.dot(hidden, w_down[0], preferred_element_type=jnp.float32).astype(jnp.bfloat16)
    returned = lax.all_to_all(
        result.reshape(received.shape), ("ep", "tp"), split_axis=0, concat_axis=0, tiled=True
    )
    picked = (
        returned[flat_ids, slot_index].reshape(tok_rows, top_count, model_width).astype(jnp.float32)
    )
    return jnp.sum(picked * route_weights[:, :, None], axis=1).astype(jnp.bfloat16)


def flipped(index, bits):
    bit = 1
    while bit <= bits:
        if bits & bit:
            index = index + (1 - 2 * ((index // bit) % 2)) * bit
        bit *= 2
    return index


PIECES = 8
EARLY = 1
AHEAD = 3
DIRECT = 3
GROUPS = ((0, 1), (1, 3), (3, 8))
DENSE_BY = ((0, 2, 3, 4, 5, 6, 7, 8), (0, 1, 2, 3, 4, 5, 6, 7, 8))
EDENSE_BY = (0, 4, 6, 8)
FAR_BY = (0, 4, 6, 7, 8)
BACK_BY = ((0, 1, 2, 3, 4, 6, 8), (0, 1, 2, 3, 5, 7, 8))
HOP_BY = (DIRECT, 4, 6, 8)
FINAL_BY = (0, 7, 8)


def span(edges, c):
    g = max(i for i in range(len(edges) - 1) if edges[i] <= c)
    return g, edges[g], edges[g + 1] - edges[g]


def slot(edges, c):
    return span(edges, c)[0]


def kernel(
    ep_count, tp_count, cap,
    x_hbm, gain_hbm, ids_hbm, wts_hbm, wg_hbm, wu_hbm, wd_hbm, out_ref,
    x_ref, gain_ref, ids_ref, wts_ref, io_sem,
    normed, meta, share_hi, share_lo, nsend, nrecv, nres, nback,
    eblock, emeta, epick, esend, hop,
    rblock, rmeta, rpick, rshare_hi, rshare_lo, fsend, frecv, fres, rback, rsend, farback,
    wg, wu, wd, acc, gate_acc, up_acc,
    w_sem, ready, dense_s, fwd_s, edense_r, dense_r, meta_s, emeta_r, meta_r, near_s, near_r,
    eout_s, lend_r, nret_s, nret_r, far_s, far_r, fret_s, fret_r, hop_s, hop_r, final_s, final_r,
):
    ep, tp, grp = lax.axis_index("ep"), lax.axis_index("tp"), lax.axis_index("grp")
    rows, width = x_ref.shape
    part_w = width // PIECES
    top = ids_ref.shape[0]
    experts = ep_count * tp_count
    near = 2 * tp_count
    me = ep * tp_count + tp
    boundary = (ep + ep // 2) % 2
    place_of_me = (1 - boundary) * tp_count
    own_relay = 1 + ep // 2
    is_boundary, is_end = boundary == 1, boundary == 0
    is_first = ep < ep_count // 2
    holds_back = jnp.logical_and(ep == ep_count // 2, tp % 2 == 0)

    def at(plane, j):
        return (grp, plane, flipped(tp, j))

    def remote(src, dst, s_sem, r_sem, target):
        return pltpu.make_async_remote_copy(
            src_ref=src, dst_ref=dst, send_sem=s_sem, recv_sem=r_sem,
            device_id=target, device_id_type=MESH,
        )

    barrier = pltpu.get_barrier_semaphore()

    def greet(target):
        pl.semaphore_signal(barrier, inc=1, device_id=target, device_id_type=MESH)

    @pl.when(is_boundary)
    def _():
        greet(at(flipped(ep, 3), 0))
        for j in range(tp_count):
            greet(at(flipped(ep, 1), j))

    @pl.when(jnp.logical_and(is_end, is_first))
    def _():
        for j in range(tp_count):
            greet(at(flipped(ep, 1), j))

    for j in range(1, tp_count):
        greet(at(ep, j))
    fetches = [
        pltpu.make_async_copy(src, dst, io_sem.at[i])
        for i, (src, dst) in enumerate((
            (x_hbm, x_ref), (gain_hbm, gain_ref), (ids_hbm, ids_ref), (wts_hbm, wts_ref)))
    ]
    for fetch in fetches:
        fetch.start()
    loads = [
        pltpu.make_async_copy(src.at[0], dst, w_sem.at[i])
        for i, (src, dst) in enumerate(((wg_hbm, wg), (wu_hbm, wu), (wd_hbm, wd)))
    ]
    partner, across_mid = flipped(ep, 1), flipped(ep, 3)

    @pl.when(is_end)
    def _():
        pl.semaphore_wait(barrier, near - 1)

    @pl.when(jnp.logical_and(is_end, jnp.logical_not(is_first)))
    def _():
        for j in range(tp_count):
            pl.semaphore_signal(ready, inc=1, device_id=at(partner, j), device_id_type=MESH)

    planes = [ep, partner]
    dense = [
        remote(normed.at[c], rblock.at[0, c], dense_s, dense_r.at[slot(DENSE_BY[0], c)], at(across_mid, 0))
        for c in range(PIECES)
    ]
    forward = [
        remote(eblock.at[c], rblock.at[1, c], fwd_s, dense_r.at[len(DENSE_BY[0]) - 1 + slot(DENSE_BY[1], c)], at(across_mid, 0))
        for c in range(PIECES)
    ]
    edense = [
        remote(normed.at[c], eblock.at[c], dense_s, edense_r.at[slot(EDENSE_BY, c)], at(partner, 0))
        for c in range(PIECES)
    ]
    far_meta = pl.ds(0, 2 * near)
    meta_copy = remote(meta.at[far_meta], rmeta.at[0], meta_s.at[0], meta_r.at[0],
                       at(across_mid, 0))
    meta_forward = remote(emeta.at[far_meta], rmeta.at[1], meta_s.at[1], meta_r.at[1],
                          at(across_mid, 0))
    emeta_copy = remote(meta, emeta, meta_s.at[0], emeta_r.at[0], at(partner, 0))
    near_out = [
        remote(nsend.at[g], nrecv.at[g], near_s, near_r.at[max(0, 2 * g // tp_count - 1)],
               at(planes[g // tp_count], g % tp_count))
        for g in range(near)
    ]
    side = tp_count // 2
    eout = [
        remote(esend.at[j], nrecv.at[tp_count + j], eout_s, near_r.at[1], at(ep, j))
        for j in range(side)
    ]
    lend = [
        remote(nsend.at[tp_count + side + k], esend.at[k], near_s, lend_r, at(ep, side))
        for k in range(side)
    ]
    pass_on = [
        remote(esend.at[k], nrecv.at[tp_count + side + k], eout_s, near_r.at[1], at(partner, k))
        for k in range(side)
    ]
    near_ret = [
        remote(nres.at[g], nback.at[g], nret_s, nret_r,
               at(planes[g // tp_count], g % tp_count))
        for g in range(near)
    ]
    far_out, far_ret, to_hop, from_hop, final = {}, {}, {}, {}, {}
    for v in range(2):
        for c in range(PIECES):
            for i in range(near):
                far_out[v, c, i] = remote(
                    fsend.at[v, c, i], frecv.at[v, c, i % tp_count], far_s,
                    far_r.at[v, slot(FAR_BY, c)], at(planes[i // tp_count], i % tp_count))
            for j in range(tp_count):
                place = place_of_me + j
                far_ret[v, c, j] = remote(
                    fres.at[v, c, j], rback.at[v, c, place], fret_s, fret_r.at[v, slot(BACK_BY[v], c)],
                    at(own_relay, j))
            if v == 0 and c >= DIRECT:
                for j in range(side, tp_count):
                    to_hop[c, j] = remote(fres.at[v, c, j], hop.at[c, j - side], fret_s,
                                          hop_r.at[slot(HOP_BY, c)], at(ep, j))
                from_hop[c] = remote(hop.at[c], rback.at[v, c, pl.ds(tp_count + side, side)],
                                     hop_s, fret_r.at[v, slot(BACK_BY[v], c)], at(own_relay, 0))
            final[v, c] = remote(rsend.at[v, c], farback.at[c], final_s, final_r.at[slot(FINAL_BY, c)],
                                 at(flipped(ep, 3 - v), 0))

    def drain(ref, sem):
        pltpu.make_async_copy(ref, ref, sem).wait()

    for fetch in fetches[:2]:
        fetch.wait()
    for load in loads:
        load.start()
    values = x_ref[...].astype(jnp.float32)
    rows_normed = (
        values
        * lax.rsqrt(jnp.mean(values * values, axis=-1, keepdims=True) + 1e-06)
        * gain_ref[...]
    ).astype(jnp.bfloat16)
    for c in range(PIECES):
        normed[c] = rows_normed[:, c * part_w:(c + 1) * part_w]

    @pl.when(is_boundary)
    def _():
        pl.semaphore_wait(barrier, tp_count + jnp.where(is_first, tp_count, 0))
        for c in range(2):
            dense[c].start()

    @pl.when(is_end)
    def _():
        for c in range(2):
            edense[c].start()

    down = lax.broadcasted_iota(jnp.int32, (rows, rows), 0)
    across = lax.broadcasted_iota(jnp.int32, (rows, rows), 1)

    expert_of = lax.broadcasted_iota(jnp.int32, (experts, rows), 0) ^ me
    for fetch in fetches[2:]:
        fetch.wait()
    ids, wts = ids_ref[...], wts_ref[...]
    named = jnp.zeros((experts, rows), jnp.float32)
    weight = jnp.zeros((experts, rows), jnp.float32)
    for k in range(top):
        match = ids[k:k + 1] == expert_of
        named = named + jnp.where(match, 1.0, 0.0)
        weight = weight + jnp.where(match, wts[k:k + 1], 0.0)
    earlier = jnp.where(down < across, 1.0, 0.0).astype(jnp.bfloat16)
    rank = jnp.dot(named.astype(jnp.bfloat16), earlier, preferred_element_type=jnp.float32)
    rank = jnp.where(named > 0.5, rank, -1.0)
    meta[0:near] = rank[near:]
    meta[near:2 * near] = weight[near:]
    meta[2 * near:] = rank[:near]

    @pl.when(is_boundary)
    def _():
        meta_copy.start()
        for c in range(2, PIECES):
            dense[c].start()

    @pl.when(is_end)
    def _():
        emeta_copy.start()
        for c in range(2, PIECES):
            edense[c].start()

    def pick_of(rank):
        count = rank.shape[0]
        slot = lax.broadcasted_iota(jnp.int32, (count, cap, rows), 1).astype(jnp.float32)
        taken = rank[:, None, :] == slot
        pick = jnp.where(taken, 1.0, 0.0).reshape(count * cap, rows).astype(jnp.bfloat16)
        return taken, pick

    def onehots(rank, weight):
        taken, pick = pick_of(rank)
        share = jnp.where(taken, weight[:, None, :], 0.0).reshape(near * cap, rows)
        high = share.astype(jnp.bfloat16)
        return pick, high, (share - high.astype(jnp.float32)).astype(jnp.bfloat16)

    pick, high, low = onehots(rank[:near], weight[:near])

    def dot(a, b):
        return jnp.dot(a, b, preferred_element_type=jnp.float32)

    half = tp_count * cap
    crossing = [*range(side, tp_count), *range(side - 1, -1, -1)]

    def pack_near(p):
        packed = dot(pick[p * half:(p + 1) * half], rows_normed)
        packed = packed.astype(jnp.bfloat16).reshape(tp_count, cap, width)
        for j in range(tp_count):
            if p or j:
                nsend[p * tp_count + j] = packed[j]
            else:
                nrecv[0] = packed[0]

    pack_near(1)

    share_hi[...] = high
    share_lo[...] = low

    def send_near(js, p=1):
        for j in js:
            near_out[p * tp_count + j].start()

    def hidden_of(gate_act, up_act):
        return (gate_act / (1.0 + jnp.exp(-gate_act)) * up_act).astype(jnp.bfloat16)

    def near_part(base, first, count, sem):
        drain(nrecv.at[pl.ds(base + first, count - first)], near_r.at[sem])
        block = nrecv[base:base + count].reshape(count * cap, width)
        hidden = hidden_of(dot(block, wg[...]), dot(block, wu[...]))
        result = dot(hidden, wd[...]).astype(jnp.bfloat16).reshape(count, cap, width)
        for j in range(count):
            if base or j:
                nres[base + j] = result[j]
            else:
                nback[0] = result[0]

    def expert_near(p, first):
        near_part(p * tp_count, first, tp_count, p)

    def return_near(gs):
        for g in gs:
            near_ret[g].start()

    def forward_end(c):
        g, lo, count = span(EDENSE_BY, c)
        if c == lo:
            drain(eblock.at[pl.ds(lo, count)], edense_r.at[g])
        forward[c].start()

    def end_meta():
        emeta_copy.wait_recv()
        meta_forward.start()
        epick[...] = pick_of(emeta[2 * near + tp_count:2 * near + tp_count + side])[1]

    def pack_end():
        for c in range(PIECES):
            packed = dot(epick[...], eblock[c]).astype(jnp.bfloat16).reshape(side, cap, part_w)
            nrecv[tp_count, :, c * part_w:(c + 1) * part_w] = packed[0]
            for j in range(1, side):
                esend[j, :, c * part_w:(c + 1) * part_w] = packed[j]
        for j in range(1, side):
            eout[j].start()

    def send_lend():
        for copy in lend:
            copy.start()

    def send_lent():
        drain(esend, lend_r)
        for copy in pass_on:
            copy.start()

    def relay_meta(v):
        remote(meta.at[far_meta], rmeta.at[v], meta_s.at[0], meta_r.at[v],
               at(across_mid, 0)).wait_recv()
        ranks, weights = rmeta[v, 0:near], rmeta[v, near:]
        if v == 0:
            ranks = jnp.concatenate([ranks[tp_count:], ranks[:tp_count]], axis=0)
            weights = jnp.concatenate([weights[tp_count:], weights[:tp_count]], axis=0)
        rp, rh, rl = onehots(ranks, weights)
        rpick[v] = rp
        rshare_hi[v] = rh
        rshare_lo[v] = rl

    def relay_out(v, c):
        g, lo, count = span(DENSE_BY[v], c)
        if c == lo:
            drain(rblock.at[v, pl.ds(lo, count)], dense_r.at[v * (len(DENSE_BY[0]) - 1) + g])
        packed = dot(rpick[v], rblock[v, c]).astype(jnp.bfloat16).reshape(near, cap, part_w)
        frecv[v, c, 0] = packed[0]
        for i in range(1, near):
            fsend[v, c, i] = packed[i]
        for i in list(range(tp_count + side, near)) + list(range(tp_count, tp_count + side)) + crossing[:-1]:
            far_out[v, c, i].start()

    def far_in(v, c, first):
        g, lo, count = span(FAR_BY, c)
        if c == lo:
            drain(frecv.at[v, pl.ds(lo, count), pl.ds(first, tp_count - first)], far_r.at[v, g])
        block = frecv[v, c].reshape(half, part_w)
        more_gate = dot(block, wg[c * part_w:(c + 1) * part_w])
        more_up = dot(block, wu[c * part_w:(c + 1) * part_w])
        gate_acc[...] = more_gate if c == 0 else gate_acc[...] + more_gate
        up_acc[...] = more_up if c == 0 else up_acc[...] + more_up

    def far_result(v, at_relay):
        hidden = hidden_of(gate_acc[...], up_acc[...])
        for lo, hi in GROUPS:
            result = dot(hidden, wd[:, lo * part_w:hi * part_w])
            result = result.astype(jnp.bfloat16).reshape(tp_count, cap, (hi - lo) * part_w)
            for c in range(lo, hi):
                part = result[:, :, (c - lo) * part_w:(c - lo + 1) * part_w]
                if at_relay:
                    rback[v, c, 0] = part[0]
                for j in range(at_relay, tp_count):
                    fres[v, c, j] = part[j]
                for j in crossing[:tp_count - at_relay]:
                    if not at_relay and (c, j) in to_hop and v == 0:
                        to_hop[c, j].start()
                    elif at_relay or v or c <= DIRECT:
                        far_ret[v, c, j].start()

    def late_return(c):
        for j in crossing[side:]:
            far_ret[0, c, j].start()

    def hop_on(c):
        g, lo, count = span(HOP_BY, c)
        if c == lo:
            drain(hop.at[pl.ds(lo, count)], hop_r.at[g])
        from_hop[c].start()

    def combine(high, low, block):
        total = None
        for comb in (high, low):
            term = lax.dot_general(
                comb, block, (((0,), (0,)), ((), ())), preferred_element_type=jnp.float32
            )
            total = term if total is None else total + term
        return total

    def relay_back(v, c):
        g, lo, count = span(BACK_BY[v], c)
        if c == lo:
            drain(rback.at[v, pl.ds(lo, count), pl.ds(1, near - 1)], fret_r.at[v, g])
        block = rback[v, c].reshape(near * cap, part_w)
        rsend[v, c] = combine(rshare_hi[v], rshare_lo[v], block).astype(jnp.bfloat16)
        final[v, c].start()

    def combine_near():
        drain(nback.at[pl.ds(1, near - 1)], nret_r)
        acc[...] = combine(share_hi[...], share_lo[...], nback[...].reshape(near * cap, width))

    def finish(c):
        g, lo, count = span(FINAL_BY, c)
        if c == lo:
            drain(farback.at[pl.ds(lo, count)], final_r.at[g])
        part = acc[:, c * part_w:(c + 1) * part_w] + farback[c].astype(jnp.float32)
        out_ref[:, c * part_w:(c + 1) * part_w] = part.astype(out_ref.dtype)

    others = range(1, tp_count)
    second = range(tp_count, near)

    def ends_here():
        @pl.when(jnp.logical_not(is_first))
        def _():
            pl.semaphore_wait(ready, tp_count)

    def weights_here():
        for load in loads:
            load.wait()

    @pl.when(is_boundary)
    def _():
        @pl.when(is_first)
        def _():
            send_near(range(AHEAD))

        pack_near(0)
        send_near(range(1, tp_count), 0)
        ends_here()

        @pl.when(jnp.logical_not(is_first))
        def _():
            send_near(range(AHEAD))

        relay_meta(0)
        last = PIECES - 1
        ahead = PIECES // 2
        for c in range(ahead):
            relay_out(0, c)
            if c == 0:
                weights_here()
                expert_near(0, 1)
                return_near(others)
        end_meta()
        for c in range(ahead - 1):
            forward_end(c)
        for c in range(ahead, PIECES):
            relay_out(0, c)
            forward_end(c - 1)
        forward_end(last)

        @pl.when(is_first)
        def _():
            send_near(range(AHEAD, tp_count))

        relay_meta(1)
        pack_end()
        relay_out(1, 0)
        for c in range(PIECES // 2):
            far_in(0, c, 1)
        relay_out(1, 1)
        for c in range(PIECES // 2, PIECES):
            far_in(0, c, 1)
        far_result(0, 1)
        relay_out(1, 2)
        relay_out(1, 3)
        expert_near(1, 1)
        relay_out(1, 4)
        relay_out(1, 5)
        relay_back(0, 0)
        relay_out(1, 6)
        relay_back(0, 1)
        relay_out(1, 7)

        @pl.when(jnp.logical_not(is_first))
        def _():
            send_near(range(AHEAD, tp_count))

        @pl.when(tp < side)
        def _():
            return_near(second)

        @pl.when(tp >= side)
        def _():
            return_near(second[::-1])

        relay_back(0, 2)
        relay_back(0, 3)
        for c in range(4):
            far_in(1, c, 1)
        relay_back(0, 4)
        for c in range(4, PIECES):
            far_in(1, c, 1)
        far_result(1, 1)
        relay_back(0, 5)
        relay_back(0, last - 1)

        @pl.when(jnp.logical_not(holds_back))
        def _():
            relay_back(0, last)

        for c in range(PIECES):
            relay_back(1, c)

        @pl.when(holds_back)
        def _():
            relay_back(0, last)

        combine_near()
        for c in range(PIECES):
            finish(c)

    @pl.when(is_end)
    def _():
        send_lend()
        pack_near(0)
        send_near(range(1, tp_count), 0)
        send_lent()
        weights_here()
        near_part(tp_count, 0, side, 1)
        return_near(list(second)[:EARLY])
        for c in range(PIECES):
            far_in(0, c, 0)
        far_result(0, 0)
        hop_on(3)
        late_return(4)
        late_return(5)
        expert_near(0, 1)
        for c in range(4):
            far_in(1, c, 0)
        hop_on(4)
        hop_on(5)
        late_return(6)
        late_return(7)
        far_in(1, 4, 0)
        far_in(1, 5, 0)
        hop_on(6)
        hop_on(7)
        far_in(1, 6, 0)
        far_in(1, 7, 0)
        far_result(1, 0)
        return_near(others)
        return_near(list(second)[EARLY:side])
        near_part(tp_count + side, 0, tp_count - side, 2)
        return_near(list(second)[side:])
        combine_near()
        for c in range(PIECES):
            finish(c)

    drain(normed, dense_s)
    drain(nres.at[pl.ds(1, near - 1)], nret_s)

    @pl.when(is_end)
    def _():
        drain(meta, meta_s.at[0])
        drain(nsend.at[pl.ds(1, tp_count + side - 1)], near_s)
        drain(esend, eout_s)
        drain(fres, fret_s)
        drain(hop.at[pl.ds(DIRECT, PIECES - DIRECT)], hop_s)

    @pl.when(is_boundary)
    def _():
        drain(meta.at[far_meta], meta_s.at[0])
        drain(meta.at[far_meta], meta_s.at[1])
        drain(eblock, fwd_s)
        drain(nsend.at[pl.ds(1, near - 1)], near_s)
        drain(esend.at[pl.ds(1, side - 1)], eout_s)
        drain(fres.at[:, :, pl.ds(1, tp_count - 1)], fret_s)
        drain(fsend.at[:, :, pl.ds(1, near - 1)], far_s)
        drain(rsend, final_s)


def fused(ep_count, tp_count, tokens, norm_gain, route_ids, route_weights, w_gate, w_up, w_down):
    rows, width = tokens.shape
    hidden = w_gate.shape[2]
    experts = ep_count * tp_count
    near = 2 * tp_count
    cap = 3 * rows * route_ids.shape[1] // (2 * experts)
    part_w = width // PIECES
    vmem = pl.BlockSpec(memory_space=pltpu.VMEM)
    hbm = pl.BlockSpec(memory_space=pltpu.HBM)

    def b16(*shape):
        return pltpu.VMEM(shape, jnp.bfloat16)

    def f32(*shape):
        return pltpu.VMEM(shape, jnp.float32)

    def sems(*shape):
        return pltpu.SemaphoreType.DMA(shape)

    one = pltpu.SemaphoreType.DMA
    return pl.pallas_call(
        functools.partial(kernel, ep_count, tp_count, cap),
        out_shape=jax.ShapeDtypeStruct((rows, width), tokens.dtype),
        in_specs=[hbm] * 7,
        out_specs=vmem,
        scratch_shapes=[
            b16(rows, width), f32(1, width),
            pltpu.VMEM(route_ids.shape[::-1], jnp.int32), f32(*route_weights.shape[::-1]), sems(4),
            b16(PIECES, rows, part_w), f32(3 * near, rows),
            b16(near * cap, rows), b16(near * cap, rows),
            *[b16(near, cap, width)] * 4,
            b16(PIECES, rows, part_w), f32(3 * near, rows),
            b16(tp_count // 2 * cap, rows), b16(tp_count // 2, cap, width),
            b16(PIECES, tp_count // 2, cap, part_w),
            b16(2, PIECES, rows, part_w), f32(2, 2 * near, rows),
            *[b16(2, near * cap, rows)] * 3,
            b16(2, PIECES, near, cap, part_w),
            b16(2, PIECES, tp_count, cap, part_w),
            b16(2, PIECES, tp_count, cap, part_w),
            b16(2, PIECES, near, cap, part_w),
            b16(2, PIECES, rows, part_w), b16(PIECES, rows, part_w),
            b16(width, hidden), b16(width, hidden), b16(hidden, width),
            f32(rows, width), f32(tp_count * cap, hidden), f32(tp_count * cap, hidden),
            sems(3), pltpu.SemaphoreType.REGULAR, one, one,
            sems(len(EDENSE_BY) - 1), sems(sum(map(len, DENSE_BY)) - 2),
            sems(2), sems(1), sems(2), one, sems(3), one, one, one, one,
            one, sems(2, len(FAR_BY) - 1), one, sems(2, len(BACK_BY[0]) - 1),
            one, sems(len(HOP_BY) - 1), one, sems(len(FINAL_BY) - 1),
        ],
        compiler_params=pltpu.CompilerParams(
            collective_id=0, has_side_effects=True, vmem_limit_bytes=32 * 1024 * 1024
        ),
    )(*(
        pltpu.with_memory_space_constraint(arg, pltpu.HBM)
        for arg in (tokens, norm_gain.reshape(1, width), route_ids.T, route_weights.T,
                    w_gate, w_up, w_down)
    ))


def solution(mesh):
    ep_count, tp_count = mesh.shape["ep"], mesh.shape["tp"]

    def on_device(*args):
        rows, experts = args[0].shape[0], ep_count * tp_count
        cap = 3 * rows * args[2].shape[1] // (2 * experts)
        if ep_count != 4 or tp_count != 4 or cap % 8 or rows % 128 or args[0].shape[1] % 256:
            return plain(*args)
        return fused(ep_count, tp_count, *args)

    return jax.shard_map(
        on_device,
        mesh=mesh,
        in_specs=(
            P(("grp", "ep", "tp"), None),
            P(),
            P(("grp", "ep", "tp"), None),
            P(("grp", "ep", "tp"), None),
            P(("ep", "tp"), None, None),
            P(("ep", "tp"), None, None),
            P(("ep", "tp"), None, None),
        ),
        out_specs=P(("grp", "ep", "tp"), None),
        check_vma=False,
    )
```

```python
import functools

import jax
import jax.numpy as jnp
from jax import lax
from jax.experimental import pallas as pl
from jax.experimental.pallas import tpu as pltpu
from jax.sharding import PartitionSpec as P

MESH = pl.DeviceIdType.MESH


def plain(tokens, norm_gain, route_ids, route_weights, w_gate, w_up, w_down):
    tok_rows, model_width = tokens.shape
    top_count = route_ids.shape[1]
    ep_count = lax.axis_size("ep")
    tp_count = lax.axis_size("tp")
    experts = ep_count * tp_count
    capacity = 3 * tok_rows * top_count // (2 * experts)
    values = tokens.astype(jnp.float32)
    normed = (
        values * lax.rsqrt(jnp.mean(values * values, axis=-1, keepdims=True) + 1e-06) * norm_gain
    ).astype(jnp.bfloat16)
    flat_ids = route_ids.reshape(-1)
    onehot = (flat_ids[:, None] == jnp.arange(experts, dtype=jnp.int32)[None, :]).astype(jnp.int32)
    slot_index = jnp.sum((jnp.cumsum(onehot, axis=0) - onehot) * onehot, axis=-1)
    token_of = jnp.arange(tok_rows * top_count, dtype=jnp.int32) // top_count
    buffer = jnp.zeros((experts, capacity, model_width), jnp.bfloat16)
    buffer = buffer.at[flat_ids, slot_index].set(normed[token_of])
    received = lax.all_to_all(buffer, ("ep", "tp"), split_axis=0, concat_axis=0, tiled=True)
    flat_rows = received.reshape(-1, model_width)
    gate_act = jnp.dot(flat_rows, w_gate[0], preferred_element_type=jnp.float32)
    up_act = jnp.dot(flat_rows, w_up[0], preferred_element_type=jnp.float32)
    hidden = (jax.nn.silu(gate_act) * up_act).astype(jnp.bfloat16)
    result = jnp.dot(hidden, w_down[0], preferred_element_type=jnp.float32).astype(jnp.bfloat16)
    returned = lax.all_to_all(
        result.reshape(received.shape), ("ep", "tp"), split_axis=0, concat_axis=0, tiled=True
    )
    picked = (
        returned[flat_ids, slot_index].reshape(tok_rows, top_count, model_width).astype(jnp.float32)
    )
    return jnp.sum(picked * route_weights[:, :, None], axis=1).astype(jnp.bfloat16)


def flipped(index, bits):
    bit = 1
    while bit <= bits:
        if bits & bit:
            index = index + (1 - 2 * ((index // bit) % 2)) * bit
        bit *= 2
    return index


PIECES = 8
EARLY = 1
AHEAD = 3
DIRECT = 3
GROUPS = ((0, 1), (1, 3), (3, 8))
DENSE_BY = ((0, 2, 3, 4, 5, 6, 7, 8), (0, 1, 2, 3, 4, 5, 6, 7, 8))
EDENSE_BY = (0, 4, 6, 8)
FAR_BY = (0, 4, 6, 7, 8)
BACK_BY = ((0, 1, 2, 3, 4, 5, 6, 8), (0, 1, 2, 3, 4, 5, 6, 7, 8))
HOP_BY = (DIRECT, 4, 6, 8)
FINAL_BY = (0, 7, 8)
WAVE_AT = (0, len(DENSE_BY[0]) - 1)


def span(edges, c):
    g = max(i for i in range(len(edges) - 1) if edges[i] <= c)
    return g, edges[g], edges[g + 1] - edges[g]


def slot(edges, c):
    return span(edges, c)[0]


def kernel(
    ep_count, tp_count, cap,
    x_hbm, gain_hbm, ids_hbm, wts_hbm, wg_hbm, wu_hbm, wd_hbm, out_ref,
    x_ref, gain_ref, ids_ref, wts_ref, io_sem,
    normed, meta, share_hi, share_lo, nsend, nrecv, nres, nback,
    eblock, emeta, epick, esend, hop,
    rblock, rmeta, rpick, rshare_hi, rshare_lo, fsend, frecv, fres, rback, rsend, farback,
    wg, wu, wd, acc, gate_acc, up_acc,
    w_sem, ready, dense_s, fwd_s, edense_r, dense_r, meta_s, emeta_r, meta_r, near_s, near_r,
    eout_s, far_s, far_r,
):
    ep, tp, grp = lax.axis_index("ep"), lax.axis_index("tp"), lax.axis_index("grp")
    rows, width = x_ref.shape
    part_w = width // PIECES
    top = ids_ref.shape[0]
    experts = ep_count * tp_count
    near = 2 * tp_count
    me = ep * tp_count + tp
    boundary = (ep + ep // 2) % 2
    place_of_me = (1 - boundary) * tp_count
    own_relay = 1 + ep // 2
    is_boundary, is_end = boundary == 1, boundary == 0
    is_first = ep < ep_count // 2
    is_late = tp % 2 == 1
    holds_back = ep == ep_count // 2

    def at(plane, j):
        return (grp, plane, flipped(tp, j))

    def remote(src, dst, s_sem, r_sem, target):
        return pltpu.make_async_remote_copy(
            src_ref=src, dst_ref=dst, send_sem=s_sem, recv_sem=r_sem,
            device_id=target, device_id_type=MESH,
        )

    barrier = pltpu.get_barrier_semaphore()

    def greet(target):
        pl.semaphore_signal(barrier, inc=1, device_id=target, device_id_type=MESH)

    @pl.when(is_boundary)
    def _():
        greet(at(flipped(ep, 3), 0))
        for j in range(tp_count):
            greet(at(flipped(ep, 1), j))

    @pl.when(jnp.logical_and(is_end, is_first))
    def _():
        for j in range(tp_count):
            greet(at(flipped(ep, 1), j))

    for j in range(1, tp_count):
        greet(at(ep, j))
    fetches = [
        pltpu.make_async_copy(src, dst, io_sem.at[i])
        for i, (src, dst) in enumerate((
            (x_hbm, x_ref), (gain_hbm, gain_ref), (ids_hbm, ids_ref), (wts_hbm, wts_ref)))
    ]
    for fetch in fetches:
        fetch.start()
    loads = [
        pltpu.make_async_copy(src.at[0], dst, w_sem.at[i])
        for i, (src, dst) in enumerate(((wg_hbm, wg), (wu_hbm, wu), (wd_hbm, wd)))
    ]
    partner, across_mid = flipped(ep, 1), flipped(ep, 3)

    @pl.when(is_end)
    def _():
        pl.semaphore_wait(barrier, near - 1)

    @pl.when(jnp.logical_and(is_end, jnp.logical_not(is_first)))
    def _():
        for j in range(tp_count):
            pl.semaphore_signal(ready, inc=1, device_id=at(partner, j), device_id_type=MESH)

    planes = [ep, partner]
    dense = [
        remote(normed.at[c], rblock.at[0, c], dense_s, dense_r.at[slot(DENSE_BY[0], c)], at(across_mid, 0))
        for c in range(PIECES)
    ]
    forward = [
        remote(eblock.at[c], rblock.at[1, c], fwd_s, dense_r.at[WAVE_AT[1] + slot(DENSE_BY[1], c)], at(across_mid, 0))
        for c in range(PIECES)
    ]
    edense = [
        remote(normed.at[c], eblock.at[c], dense_s, edense_r.at[slot(EDENSE_BY, c)], at(partner, 0))
        for c in range(PIECES)
    ]
    far_meta = pl.ds(0, 2 * near)
    meta_copy = remote(meta.at[far_meta], rmeta.at[0], meta_s, meta_r.at[0],
                       at(across_mid, 0))
    meta_forward = remote(emeta.at[far_meta], rmeta.at[1], meta_s, meta_r.at[1],
                          at(across_mid, 0))
    emeta_copy = remote(meta, emeta, meta_s, emeta_r.at[0], at(partner, 0))
    near_out = [
        remote(nsend.at[g], nrecv.at[g], near_s, near_r.at[max(0, 2 * g // tp_count - 1)],
               at(planes[g // tp_count], g % tp_count))
        for g in range(near)
    ]
    side = tp_count // 2
    eout = [
        remote(esend.at[j], nrecv.at[tp_count + j], eout_s, near_r.at[1], at(ep, j))
        for j in range(side)
    ]
    lend = [
        remote(nsend.at[tp_count + side + k], esend.at[k], near_s, dense_r.at[len(HOP_BY)], at(ep, side))
        for k in range(side)
    ]
    pass_on = [
        remote(esend.at[k], nrecv.at[tp_count + side + k], eout_s, near_r.at[1], at(partner, k))
        for k in range(side)
    ]
    near_ret = [
        remote(nres.at[g], nback.at[g], w_sem.at[0], io_sem.at[2 + g // tp_count],
               at(planes[g // tp_count], g % tp_count))
        for g in range(near)
    ]
    far_out, far_ret, to_hop, from_hop, final = {}, {}, {}, {}, {}
    for v in range(2):
        for c in range(PIECES):
            for i in range(near):
                far_out[v, c, i] = remote(
                    fsend.at[v, c, i], frecv.at[v, c, i % tp_count], far_s,
                    far_r.at[v, slot(FAR_BY, c)], at(planes[i // tp_count], i % tp_count))
            for j in range(tp_count):
                place = place_of_me + j
                far_ret[v, c, j] = remote(
                    fres.at[v, c, j], rback.at[v, c, place], w_sem.at[1], dense_r.at[WAVE_AT[v] + slot(BACK_BY[v], c)],
                    at(own_relay, j))
            if v == 0 and c >= DIRECT:
                for j in range(side, tp_count):
                    to_hop[c, j] = remote(fres.at[v, c, j], hop.at[c, j - side], w_sem.at[1],
                                          dense_r.at[slot(HOP_BY, c)], at(ep, j))
                from_hop[c] = remote(hop.at[c], rback.at[v, c, pl.ds(tp_count + side, side)],
                                     fwd_s, dense_r.at[WAVE_AT[v] + slot(BACK_BY[v], c)], at(own_relay, 0))
            final[v, c] = remote(rsend.at[v, c], farback.at[c], w_sem.at[2], io_sem.at[slot(FINAL_BY, c)],
                                 at(flipped(ep, 3 - v), 0))

    def drain(ref, sem):
        pltpu.make_async_copy(ref, ref, sem).wait()

    for fetch in fetches[:2]:
        fetch.wait()
    for load in loads:
        load.start()
    values = x_ref[...].astype(jnp.float32)
    rows_normed = (
        values
        * lax.rsqrt(jnp.mean(values * values, axis=-1, keepdims=True) + 1e-06)
        * gain_ref[...]
    ).astype(jnp.bfloat16)
    for c in range(PIECES):
        normed[c] = rows_normed[:, c * part_w:(c + 1) * part_w]

    @pl.when(is_boundary)
    def _():
        pl.semaphore_wait(barrier, tp_count + jnp.where(is_first, tp_count, 0))
        for c in range(2):
            dense[c].start()

    @pl.when(is_end)
    def _():
        for c in range(2):
            edense[c].start()

    down = lax.broadcasted_iota(jnp.int32, (rows, rows), 0)
    across = lax.broadcasted_iota(jnp.int32, (rows, rows), 1)

    expert_of = lax.broadcasted_iota(jnp.int32, (experts, rows), 0) ^ me
    for fetch in fetches[2:]:
        fetch.wait()
    ids, wts = ids_ref[...], wts_ref[...]
    named = jnp.zeros((experts, rows), jnp.float32)
    weight = jnp.zeros((experts, rows), jnp.float32)
    for k in range(top):
        match = ids[k:k + 1] == expert_of
        named = named + jnp.where(match, 1.0, 0.0)
        weight = weight + jnp.where(match, wts[k:k + 1], 0.0)
    earlier = jnp.where(down < across, 1.0, 0.0).astype(jnp.bfloat16)
    rank = jnp.dot(named.astype(jnp.bfloat16), earlier, preferred_element_type=jnp.float32)
    rank = jnp.where(named > 0.5, rank, -1.0)
    meta[0:near] = rank[near:]
    meta[near:2 * near] = weight[near:]
    meta[2 * near:] = rank[:near]

    @pl.when(is_boundary)
    def _():
        meta_copy.start()
        for c in range(2, PIECES):
            dense[c].start()

    @pl.when(is_end)
    def _():
        emeta_copy.start()
        for c in range(2, PIECES):
            edense[c].start()

    def pick_of(rank):
        count = rank.shape[0]
        slot = lax.broadcasted_iota(jnp.int32, (count, cap, rows), 1).astype(jnp.float32)
        taken = rank[:, None, :] == slot
        pick = jnp.where(taken, 1.0, 0.0).reshape(count * cap, rows).astype(jnp.bfloat16)
        return taken, pick

    def onehots(rank, weight):
        taken, pick = pick_of(rank)
        share = jnp.where(taken, weight[:, None, :], 0.0).reshape(near * cap, rows)
        high = share.astype(jnp.bfloat16)
        return pick, high, (share - high.astype(jnp.float32)).astype(jnp.bfloat16)

    pick, high, low = onehots(rank[:near], weight[:near])

    def dot(a, b):
        return jnp.dot(a, b, preferred_element_type=jnp.float32)

    half = tp_count * cap
    crossing = [*range(side, tp_count), *range(side - 1, -1, -1)]

    def pack_near(p):
        packed = dot(pick[p * half:(p + 1) * half], rows_normed)
        packed = packed.astype(jnp.bfloat16).reshape(tp_count, cap, width)
        for j in range(tp_count):
            if p or j:
                nsend[p * tp_count + j] = packed[j]
            else:
                nrecv[0] = packed[0]

    pack_near(1)

    share_hi[...] = high
    share_lo[...] = low

    def send_near(js, p=1):
        for j in js:
            near_out[p * tp_count + j].start()

    def hidden_of(gate_act, up_act):
        return (gate_act / (1.0 + jnp.exp(-gate_act)) * up_act).astype(jnp.bfloat16)

    def near_part(base, first, count, sem):
        drain(nrecv.at[pl.ds(base + first, count - first)], near_r.at[sem])
        block = nrecv[base:base + count].reshape(count * cap, width)
        hidden = hidden_of(dot(block, wg[...]), dot(block, wu[...]))
        result = dot(hidden, wd[...]).astype(jnp.bfloat16).reshape(count, cap, width)
        for j in range(count):
            if base or j:
                nres[base + j] = result[j]
            else:
                nback[0] = result[0]

    def expert_near(p, first):
        near_part(p * tp_count, first, tp_count, p)

    def return_near(gs):
        for g in gs:
            near_ret[g].start()

    def forward_end(c):
        g, lo, count = span(EDENSE_BY, c)
        if c == lo:
            drain(eblock.at[pl.ds(lo, count)], edense_r.at[g])
        forward[c].start()

    def end_meta():
        emeta_copy.wait_recv()
        meta_forward.start()
        epick[...] = pick_of(emeta[2 * near + tp_count:2 * near + tp_count + side])[1]

    def pack_end():
        for c in range(PIECES):
            packed = dot(epick[...], eblock[c]).astype(jnp.bfloat16).reshape(side, cap, part_w)
            nrecv[tp_count, :, c * part_w:(c + 1) * part_w] = packed[0]
            for j in range(1, side):
                esend[j, :, c * part_w:(c + 1) * part_w] = packed[j]
        for j in range(1, side):
            eout[j].start()

    def send_lend():
        for copy in lend:
            copy.start()

    def send_lent():
        drain(esend, dense_r.at[len(HOP_BY)])
        for copy in pass_on:
            copy.start()

    def relay_meta(v):
        remote(meta.at[far_meta], rmeta.at[v], meta_s, meta_r.at[v],
               at(across_mid, 0)).wait_recv()
        ranks, weights = rmeta[v, 0:near], rmeta[v, near:]
        if v == 0:
            ranks = jnp.concatenate([ranks[tp_count:], ranks[:tp_count]], axis=0)
            weights = jnp.concatenate([weights[tp_count:], weights[:tp_count]], axis=0)
        rp, rh, rl = onehots(ranks, weights)
        rpick[v] = rp
        rshare_hi[v] = rh
        rshare_lo[v] = rl

    def relay_out(v, c):
        g, lo, count = span(DENSE_BY[v], c)
        if c == lo:
            drain(rblock.at[v, pl.ds(lo, count)], dense_r.at[WAVE_AT[v] + g])
        packed = dot(rpick[v], rblock[v, c]).astype(jnp.bfloat16).reshape(near, cap, part_w)
        frecv[v, c, 0] = packed[0]
        for i in range(1, near):
            fsend[v, c, i] = packed[i]
        for i in list(range(tp_count + side, near)) + list(range(tp_count, tp_count + side)) + crossing[:-1]:
            far_out[v, c, i].start()

    def far_in(v, c, first):
        g, lo, count = span(FAR_BY, c)
        if c == lo:
            drain(frecv.at[v, pl.ds(lo, count), pl.ds(first, tp_count - first)], far_r.at[v, g])
        block = frecv[v, c].reshape(half, part_w)
        more_gate = dot(block, wg[c * part_w:(c + 1) * part_w])
        more_up = dot(block, wu[c * part_w:(c + 1) * part_w])
        gate_acc[...] = more_gate if c == 0 else gate_acc[...] + more_gate
        up_acc[...] = more_up if c == 0 else up_acc[...] + more_up

    def far_result(v, at_relay):
        hidden = hidden_of(gate_acc[...], up_acc[...])
        for lo, hi in GROUPS:
            result = dot(hidden, wd[:, lo * part_w:hi * part_w])
            result = result.astype(jnp.bfloat16).reshape(tp_count, cap, (hi - lo) * part_w)
            for c in range(lo, hi):
                part = result[:, :, (c - lo) * part_w:(c - lo + 1) * part_w]
                if at_relay:
                    rback[v, c, 0] = part[0]
                for j in range(at_relay, tp_count):
                    fres[v, c, j] = part[j]
                for j in crossing[:tp_count - at_relay]:
                    if not at_relay and (c, j) in to_hop and v == 0:
                        to_hop[c, j].start()
                    elif at_relay or v or c <= DIRECT:
                        far_ret[v, c, j].start()

    def late_return(c):
        for j in crossing[side:]:
            far_ret[0, c, j].start()

    def hop_on(c):
        g, lo, count = span(HOP_BY, c)
        if c == lo:
            drain(hop.at[pl.ds(lo, count)], dense_r.at[g])
        from_hop[c].start()

    def combine(high, low, block):
        total = None
        for comb in (high, low):
            term = lax.dot_general(
                comb, block, (((0,), (0,)), ((), ())), preferred_element_type=jnp.float32
            )
            total = term if total is None else total + term
        return total

    def relay_back(v, c):
        g, lo, count = span(BACK_BY[v], c)
        if c == lo:
            drain(rback.at[v, pl.ds(lo, count), pl.ds(1, near - 1)], dense_r.at[WAVE_AT[v] + g])
        block = rback[v, c].reshape(near * cap, part_w)
        rsend[v, c] = combine(rshare_hi[v], rshare_lo[v], block).astype(jnp.bfloat16)
        final[v, c].start()

    def combine_near():
        for p in range(2):
            lo = p * half
            first = p * tp_count + 1 - p
            drain(nback.at[pl.ds(first, tp_count - 1 + p)], io_sem.at[2 + p])
            block = nback[p * tp_count:(p + 1) * tp_count].reshape(half, width)
            part = combine(share_hi[lo:lo + half], share_lo[lo:lo + half], block)
            acc[...] = acc[...] + part if p else part

    def finish(c):
        g, lo, count = span(FINAL_BY, c)
        if c == lo:
            drain(farback.at[pl.ds(lo, count)], io_sem.at[g])
        part = acc[:, c * part_w:(c + 1) * part_w] + farback[c].astype(jnp.float32)
        out_ref[:, c * part_w:(c + 1) * part_w] = part.astype(out_ref.dtype)

    others = range(1, tp_count)
    second = range(tp_count, near)

    def ends_here():
        @pl.when(jnp.logical_not(is_first))
        def _():
            pl.semaphore_wait(ready, tp_count)

    def weights_here():
        for load in loads:
            load.wait()

    @pl.when(is_boundary)
    def _():
        @pl.when(is_first)
        def _():
            send_near(range(AHEAD))

        pack_near(0)
        send_near(range(1, tp_count), 0)
        ends_here()

        @pl.when(jnp.logical_not(is_first))
        def _():
            send_near(range(AHEAD - 1))

        @pl.when(jnp.logical_not(jnp.logical_or(is_first, is_late)))
        def _():
            send_near([AHEAD - 1])

        relay_meta(0)
        last = PIECES - 1
        ahead = PIECES // 2
        for c in range(ahead):
            relay_out(0, c)
            if c == 0:
                weights_here()
                expert_near(0, 1)
                return_near(others)
        end_meta()
        for c in range(ahead - 1):
            forward_end(c)
        for c in range(ahead, PIECES):
            relay_out(0, c)
            forward_end(c - 1)
        forward_end(last)

        @pl.when(is_first)
        def _():
            send_near(range(AHEAD, tp_count))

        @pl.when(jnp.logical_and(jnp.logical_not(is_first), is_late))
        def _():
            send_near([AHEAD - 1])

        relay_meta(1)
        pack_end()
        relay_out(1, 0)
        for c in range(PIECES // 2):
            far_in(0, c, 1)
        relay_out(1, 1)
        for c in range(PIECES // 2, PIECES):
            far_in(0, c, 1)
        far_result(0, 1)
        relay_out(1, 2)
        relay_out(1, 3)
        expert_near(1, 1)
        relay_out(1, 4)
        relay_out(1, 5)
        relay_back(0, 0)
        relay_out(1, 6)
        relay_back(0, 1)
        relay_out(1, 7)

        @pl.when(jnp.logical_not(is_first))
        def _():
            send_near(range(AHEAD, tp_count))

        @pl.when(tp < side)
        def _():
            return_near(second)

        @pl.when(tp >= side)
        def _():
            return_near(second[::-1])

        relay_back(0, 2)
        relay_back(0, 3)
        for c in range(4):
            far_in(1, c, 1)
        relay_back(0, 4)
        for c in range(4, PIECES):
            far_in(1, c, 1)
        far_result(1, 1)
        relay_back(0, 5)
        relay_back(0, last - 1)

        @pl.when(jnp.logical_not(holds_back))
        def _():
            relay_back(0, last)

        for c in range(PIECES):
            relay_back(1, c)

        @pl.when(holds_back)
        def _():
            relay_back(0, last)

        combine_near()
        for c in range(PIECES):
            finish(c)

    @pl.when(is_end)
    def _():
        send_lend()
        pack_near(0)
        send_near(range(1, tp_count), 0)
        send_lent()
        weights_here()
        near_part(tp_count, 0, side, 1)
        return_near(list(second)[:EARLY])
        for c in range(PIECES):
            far_in(0, c, 0)
        far_result(0, 0)
        hop_on(3)
        late_return(4)
        late_return(5)
        expert_near(0, 1)
        for c in range(4):
            far_in(1, c, 0)
        hop_on(4)
        hop_on(5)
        late_return(6)
        late_return(7)
        far_in(1, 4, 0)
        far_in(1, 5, 0)
        hop_on(6)
        hop_on(7)
        far_in(1, 6, 0)
        far_in(1, 7, 0)
        far_result(1, 0)
        return_near(others)
        return_near(list(second)[EARLY:side])
        near_part(tp_count + side, 0, tp_count - side, 2)
        return_near(list(second)[side:])
        combine_near()
        for c in range(PIECES):
            finish(c)

    drain(normed, dense_s)
    drain(nres.at[pl.ds(1, near - 1)], w_sem.at[0])

    @pl.when(is_end)
    def _():
        drain(meta, meta_s)
        drain(nsend.at[pl.ds(1, tp_count + side - 1)], near_s)
        drain(esend, eout_s)
        drain(fres, w_sem.at[1])
        drain(hop.at[pl.ds(DIRECT, PIECES - DIRECT)], fwd_s)

    @pl.when(is_boundary)
    def _():
        drain(rmeta, meta_s)
        drain(eblock, fwd_s)
        drain(nsend.at[pl.ds(1, near - 1)], near_s)
        drain(esend.at[pl.ds(1, side - 1)], eout_s)
        drain(fres.at[:, :, pl.ds(1, tp_count - 1)], w_sem.at[1])
        drain(fsend.at[:, :, pl.ds(1, near - 1)], far_s)
        drain(rsend, w_sem.at[2])


def fused(ep_count, tp_count, tokens, norm_gain, route_ids, route_weights, w_gate, w_up, w_down):
    rows, width = tokens.shape
    hidden = w_gate.shape[2]
    experts = ep_count * tp_count
    near = 2 * tp_count
    cap = 3 * rows * route_ids.shape[1] // (2 * experts)
    part_w = width // PIECES
    vmem = pl.BlockSpec(memory_space=pltpu.VMEM)
    hbm = pl.BlockSpec(memory_space=pltpu.HBM)

    def b16(*shape):
        return pltpu.VMEM(shape, jnp.bfloat16)

    def f32(*shape):
        return pltpu.VMEM(shape, jnp.float32)

    def sems(*shape):
        return pltpu.SemaphoreType.DMA(shape)

    one = pltpu.SemaphoreType.DMA
    return pl.pallas_call(
        functools.partial(kernel, ep_count, tp_count, cap),
        out_shape=jax.ShapeDtypeStruct((rows, width), tokens.dtype),
        in_specs=[hbm] * 7,
        out_specs=vmem,
        scratch_shapes=[
            b16(rows, width), f32(1, width),
            pltpu.VMEM(route_ids.shape[::-1], jnp.int32), f32(*route_weights.shape[::-1]), sems(4),
            b16(PIECES, rows, part_w), f32(3 * near, rows),
            b16(near * cap, rows), b16(near * cap, rows),
            *[b16(near, cap, width)] * 4,
            b16(PIECES, rows, part_w), f32(3 * near, rows),
            b16(tp_count // 2 * cap, rows), b16(tp_count // 2, cap, width),
            b16(PIECES, tp_count // 2, cap, part_w),
            b16(2, PIECES, rows, part_w), f32(2, 2 * near, rows),
            *[b16(2, near * cap, rows)] * 3,
            b16(2, PIECES, near, cap, part_w),
            b16(2, PIECES, tp_count, cap, part_w),
            b16(2, PIECES, tp_count, cap, part_w),
            b16(2, PIECES, near, cap, part_w),
            b16(2, PIECES, rows, part_w), b16(PIECES, rows, part_w),
            b16(width, hidden), b16(width, hidden), b16(hidden, width),
            f32(rows, width), f32(tp_count * cap, hidden), f32(tp_count * cap, hidden),
            sems(3), pltpu.SemaphoreType.REGULAR, one, one,
            sems(len(EDENSE_BY) - 1), sems(sum(map(len, DENSE_BY)) - 2),
            one, sems(1), sems(2), one, sems(3), one, one, sems(2, len(FAR_BY) - 1),
        ],
        compiler_params=pltpu.CompilerParams(
            collective_id=0, has_side_effects=True, vmem_limit_bytes=32 * 1024 * 1024
        ),
    )(*(
        pltpu.with_memory_space_constraint(arg, pltpu.HBM)
        for arg in (tokens, norm_gain.reshape(1, width), route_ids.T, route_weights.T,
                    w_gate, w_up, w_down)
    ))


def solution(mesh):
    ep_count, tp_count = mesh.shape["ep"], mesh.shape["tp"]

    def on_device(*args):
        rows, experts = args[0].shape[0], ep_count * tp_count
        cap = 3 * rows * args[2].shape[1] // (2 * experts)
        if ep_count != 4 or tp_count != 4 or cap % 8 or rows % 128 or args[0].shape[1] % 256:
            return plain(*args)
        return fused(ep_count, tp_count, *args)

    return jax.shard_map(
        on_device,
        mesh=mesh,
        in_specs=(
            P(("grp", "ep", "tp"), None),
            P(),
            P(("grp", "ep", "tp"), None),
            P(("grp", "ep", "tp"), None),
            P(("ep", "tp"), None, None),
            P(("ep", "tp"), None, None),
            P(("ep", "tp"), None, None),
        ),
        out_specs=P(("grp", "ep", "tp"), None),
        check_vma=False,
    )
```

```python
import functools

import jax
import jax.numpy as jnp
from jax import lax
from jax.experimental import pallas as pl
from jax.experimental.pallas import tpu as pltpu
from jax.sharding import PartitionSpec as P

MESH = pl.DeviceIdType.MESH


def plain(tokens, norm_gain, route_ids, route_weights, w_gate, w_up, w_down):
    tok_rows, model_width = tokens.shape
    top_count = route_ids.shape[1]
    ep_count = lax.axis_size("ep")
    tp_count = lax.axis_size("tp")
    experts = ep_count * tp_count
    capacity = 3 * tok_rows * top_count // (2 * experts)
    values = tokens.astype(jnp.float32)
    normed = (
        values * lax.rsqrt(jnp.mean(values * values, axis=-1, keepdims=True) + 1e-06) * norm_gain
    ).astype(jnp.bfloat16)
    flat_ids = route_ids.reshape(-1)
    onehot = (flat_ids[:, None] == jnp.arange(experts, dtype=jnp.int32)[None, :]).astype(jnp.int32)
    slot_index = jnp.sum((jnp.cumsum(onehot, axis=0) - onehot) * onehot, axis=-1)
    token_of = jnp.arange(tok_rows * top_count, dtype=jnp.int32) // top_count
    buffer = jnp.zeros((experts, capacity, model_width), jnp.bfloat16)
    buffer = buffer.at[flat_ids, slot_index].set(normed[token_of])
    received = lax.all_to_all(buffer, ("ep", "tp"), split_axis=0, concat_axis=0, tiled=True)
    flat_rows = received.reshape(-1, model_width)
    gate_act = jnp.dot(flat_rows, w_gate[0], preferred_element_type=jnp.float32)
    up_act = jnp.dot(flat_rows, w_up[0], preferred_element_type=jnp.float32)
    hidden = (jax.nn.silu(gate_act) * up_act).astype(jnp.bfloat16)
    result = jnp.dot(hidden, w_down[0], preferred_element_type=jnp.float32).astype(jnp.bfloat16)
    returned = lax.all_to_all(
        result.reshape(received.shape), ("ep", "tp"), split_axis=0, concat_axis=0, tiled=True
    )
    picked = (
        returned[flat_ids, slot_index].reshape(tok_rows, top_count, model_width).astype(jnp.float32)
    )
    return jnp.sum(picked * route_weights[:, :, None], axis=1).astype(jnp.bfloat16)


def flipped(index, bits):
    bit = 1
    while bit <= bits:
        if bits & bit:
            index = index + (1 - 2 * ((index // bit) % 2)) * bit
        bit *= 2
    return index


PIECES = 8
EARLY = 1
AHEAD = 3
DIRECT = 3
PACED = 4
GROUPS = ((0, 1), (1, 3), (3, 8))
DENSE_BY = ((0, 2, 3, 4, 5, 6, 7, 8), (0, 1, 2, 3, 4, 5, 6, 7, 8))
EDENSE_BY = (0, 4, 6, 8)
FAR_BY = (0, 4, 6, 7, 8)
BACK_BY = ((0, 1, 2, 3, 4, 5, 6, 8), (0, 1, 2, 3, 4, 5, 6, 7, 8))
HOP_BY = (DIRECT, 4, 6, 8)
FINAL_BY = (0, 7, 8)
WAVE_AT = (0, len(DENSE_BY[0]) - 1)


def span(edges, c):
    g = max(i for i in range(len(edges) - 1) if edges[i] <= c)
    return g, edges[g], edges[g + 1] - edges[g]


def slot(edges, c):
    return span(edges, c)[0]


def kernel(
    ep_count, tp_count, cap,
    x_hbm, gain_hbm, ids_hbm, wts_hbm, wg_hbm, wu_hbm, wd_hbm, out_ref,
    x_ref, gain_ref, ids_ref, wts_ref, io_sem,
    normed, meta, share_hi, share_lo, nsend, nrecv, nres, nback,
    eblock, emeta, epick, esend, hop,
    rblock, rmeta, rpick, rshare_hi, rshare_lo, fsend, frecv, fres, rback, rsend, farback,
    wg, wu, wd, acc, gate_acc, up_acc,
    w_sem, ready, dense_s, fwd_s, edense_r, dense_r, meta_s, emeta_r, meta_r, near_s, near_r,
    eout_s, far_s, far_r,
):
    ep, tp, grp = lax.axis_index("ep"), lax.axis_index("tp"), lax.axis_index("grp")
    rows, width = x_ref.shape
    part_w = width // PIECES
    top = ids_ref.shape[0]
    experts = ep_count * tp_count
    near = 2 * tp_count
    me = ep * tp_count + tp
    boundary = (ep + ep // 2) % 2
    place_of_me = (1 - boundary) * tp_count
    own_relay = 1 + ep // 2
    is_boundary, is_end = boundary == 1, boundary == 0
    is_first = ep < ep_count // 2
    is_late = tp % 2 == 1
    holds_back = ep == ep_count // 2

    def at(plane, j):
        return (grp, plane, flipped(tp, j))

    def remote(src, dst, s_sem, r_sem, target):
        return pltpu.make_async_remote_copy(
            src_ref=src, dst_ref=dst, send_sem=s_sem, recv_sem=r_sem,
            device_id=target, device_id_type=MESH,
        )

    barrier = pltpu.get_barrier_semaphore()

    def greet(target):
        pl.semaphore_signal(barrier, inc=1, device_id=target, device_id_type=MESH)

    @pl.when(is_boundary)
    def _():
        greet(at(flipped(ep, 3), 0))
        for j in range(tp_count):
            greet(at(flipped(ep, 1), j))

    @pl.when(jnp.logical_and(is_end, is_first))
    def _():
        for j in range(tp_count):
            greet(at(flipped(ep, 1), j))

    for j in range(1, tp_count):
        greet(at(ep, j))
    fetches = [
        pltpu.make_async_copy(src, dst, io_sem.at[i])
        for i, (src, dst) in enumerate((
            (x_hbm, x_ref), (gain_hbm, gain_ref), (ids_hbm, ids_ref), (wts_hbm, wts_ref)))
    ]
    for fetch in fetches:
        fetch.start()
    loads = [
        pltpu.make_async_copy(src.at[0], dst, w_sem.at[i])
        for i, (src, dst) in enumerate(((wg_hbm, wg), (wu_hbm, wu), (wd_hbm, wd)))
    ]
    partner, across_mid = flipped(ep, 1), flipped(ep, 3)

    @pl.when(is_end)
    def _():
        pl.semaphore_wait(barrier, near - 1)

    @pl.when(jnp.logical_and(is_end, jnp.logical_not(is_first)))
    def _():
        for j in range(tp_count):
            pl.semaphore_signal(ready, inc=1, device_id=at(partner, j), device_id_type=MESH)

    planes = [ep, partner]
    dense = [
        remote(normed.at[c], rblock.at[0, c], dense_s, dense_r.at[slot(DENSE_BY[0], c)], at(across_mid, 0))
        for c in range(PIECES)
    ]
    forward = [
        remote(eblock.at[c], rblock.at[1, c], fwd_s, dense_r.at[WAVE_AT[1] + slot(DENSE_BY[1], c)], at(across_mid, 0))
        for c in range(PIECES)
    ]
    edense = [
        remote(normed.at[c], eblock.at[c], dense_s, edense_r.at[slot(EDENSE_BY, c)], at(partner, 0))
        for c in range(PIECES)
    ]
    far_meta = pl.ds(0, 2 * near)
    meta_copy = remote(meta.at[far_meta], rmeta.at[0], meta_s, meta_r.at[0],
                       at(across_mid, 0))
    meta_forward = remote(emeta.at[far_meta], rmeta.at[1], meta_s, meta_r.at[1],
                          at(across_mid, 0))
    emeta_copy = remote(meta, emeta, meta_s, emeta_r.at[0], at(partner, 0))
    near_out = [
        remote(nsend.at[g], nrecv.at[g], near_s, near_r.at[max(0, 2 * g // tp_count - 1)],
               at(planes[g // tp_count], g % tp_count))
        for g in range(near)
    ]
    side = tp_count // 2
    eout = [
        remote(esend.at[j], nrecv.at[tp_count + j], eout_s, near_r.at[1], at(ep, j))
        for j in range(side)
    ]
    lend = [
        remote(nsend.at[tp_count + side + k], esend.at[k], near_s, dense_r.at[len(HOP_BY)], at(ep, side))
        for k in range(side)
    ]
    pass_on = [
        remote(esend.at[k], nrecv.at[tp_count + side + k], eout_s, near_r.at[1], at(partner, k))
        for k in range(side)
    ]
    near_ret = [
        remote(nres.at[g], nback.at[g], w_sem.at[0], io_sem.at[2 + g // tp_count],
               at(planes[g // tp_count], g % tp_count))
        for g in range(near)
    ]
    far_out, far_ret, to_hop, from_hop, final = {}, {}, {}, {}, {}
    for v in range(2):
        for c in range(PIECES):
            for i in range(near):
                far_out[v, c, i] = remote(
                    fsend.at[v, c, i], frecv.at[v, c, i % tp_count], far_s,
                    far_r.at[v, slot(FAR_BY, c)], at(planes[i // tp_count], i % tp_count))
            for j in range(tp_count):
                place = place_of_me + j
                far_ret[v, c, j] = remote(
                    fres.at[v, c, j], rback.at[v, c, place], w_sem.at[1], dense_r.at[WAVE_AT[v] + slot(BACK_BY[v], c)],
                    at(own_relay, j))
            if v == 0 and c >= DIRECT:
                for j in range(side, tp_count):
                    to_hop[c, j] = remote(fres.at[v, c, j], hop.at[c, j - side], w_sem.at[1],
                                          dense_r.at[slot(HOP_BY, c)], at(ep, j))
                from_hop[c] = remote(hop.at[c], rback.at[v, c, pl.ds(tp_count + side, side)],
                                     fwd_s, dense_r.at[WAVE_AT[v] + slot(BACK_BY[v], c)], at(own_relay, 0))
            final[v, c] = remote(rsend.at[v, c], farback.at[c], w_sem.at[2], io_sem.at[slot(FINAL_BY, c)],
                                 at(flipped(ep, 3 - v), 0))

    def drain(ref, sem):
        pltpu.make_async_copy(ref, ref, sem).wait()

    for fetch in fetches[:2]:
        fetch.wait()
    for load in loads:
        load.start()
    values = x_ref[...].astype(jnp.float32)
    rows_normed = (
        values
        * lax.rsqrt(jnp.mean(values * values, axis=-1, keepdims=True) + 1e-06)
        * gain_ref[...]
    ).astype(jnp.bfloat16)
    for c in range(PIECES):
        normed[c] = rows_normed[:, c * part_w:(c + 1) * part_w]

    @pl.when(is_boundary)
    def _():
        pl.semaphore_wait(barrier, tp_count + jnp.where(is_first, tp_count, 0))
        for c in range(2):
            dense[c].start()

    @pl.when(is_end)
    def _():
        for c in range(2):
            edense[c].start()

    down = lax.broadcasted_iota(jnp.int32, (rows, rows), 0)
    across = lax.broadcasted_iota(jnp.int32, (rows, rows), 1)

    expert_of = lax.broadcasted_iota(jnp.int32, (experts, rows), 0) ^ me
    for fetch in fetches[2:]:
        fetch.wait()
    ids, wts = ids_ref[...], wts_ref[...]
    named = jnp.zeros((experts, rows), jnp.float32)
    weight = jnp.zeros((experts, rows), jnp.float32)
    for k in range(top):
        match = ids[k:k + 1] == expert_of
        named = named + jnp.where(match, 1.0, 0.0)
        weight = weight + jnp.where(match, wts[k:k + 1], 0.0)
    earlier = jnp.where(down < across, 1.0, 0.0).astype(jnp.bfloat16)
    rank = jnp.dot(named.astype(jnp.bfloat16), earlier, preferred_element_type=jnp.float32)
    rank = jnp.where(named > 0.5, rank, -1.0)
    meta[0:near] = rank[near:]
    meta[near:2 * near] = weight[near:]
    meta[2 * near:] = rank[:near]

    @pl.when(is_boundary)
    def _():
        meta_copy.start()
        for c in range(2, PIECES):
            dense[c].start()

    @pl.when(is_end)
    def _():
        emeta_copy.start()
        for c in range(2, PIECES):
            edense[c].start()

    def pick_of(rank):
        count = rank.shape[0]
        slot = lax.broadcasted_iota(jnp.int32, (count, cap, rows), 1).astype(jnp.float32)
        taken = rank[:, None, :] == slot
        pick = jnp.where(taken, 1.0, 0.0).reshape(count * cap, rows).astype(jnp.bfloat16)
        return taken, pick

    def onehots(rank, weight):
        taken, pick = pick_of(rank)
        share = jnp.where(taken, weight[:, None, :], 0.0).reshape(near * cap, rows)
        high = share.astype(jnp.bfloat16)
        return pick, high, (share - high.astype(jnp.float32)).astype(jnp.bfloat16)

    pick, high, low = onehots(rank[:near], weight[:near])

    def dot(a, b):
        return jnp.dot(a, b, preferred_element_type=jnp.float32)

    half = tp_count * cap
    crossing = [*range(side, tp_count), *range(side - 1, -1, -1)]

    def pack_near(p):
        packed = dot(pick[p * half:(p + 1) * half], rows_normed)
        packed = packed.astype(jnp.bfloat16).reshape(tp_count, cap, width)
        for j in range(tp_count):
            if p or j:
                nsend[p * tp_count + j] = packed[j]
            else:
                nrecv[0] = packed[0]

    pack_near(1)

    share_hi[...] = high
    share_lo[...] = low

    def send_near(js, p=1):
        for j in js:
            near_out[p * tp_count + j].start()

    def hidden_of(gate_act, up_act):
        return (gate_act / (1.0 + jnp.exp(-gate_act)) * up_act).astype(jnp.bfloat16)

    def near_part(base, first, count, sem):
        drain(nrecv.at[pl.ds(base + first, count - first)], near_r.at[sem])
        block = nrecv[base:base + count].reshape(count * cap, width)
        hidden = hidden_of(dot(block, wg[...]), dot(block, wu[...]))
        result = dot(hidden, wd[...]).astype(jnp.bfloat16).reshape(count, cap, width)
        for j in range(count):
            if base or j:
                nres[base + j] = result[j]
            else:
                nback[0] = result[0]

    def expert_near(p, first):
        near_part(p * tp_count, first, tp_count, p)

    def return_near(gs):
        for g in gs:
            near_ret[g].start()

    def forward_end(c):
        g, lo, count = span(EDENSE_BY, c)
        if c == lo:
            drain(eblock.at[pl.ds(lo, count)], edense_r.at[g])
        forward[c].start()

    def end_meta():
        emeta_copy.wait_recv()
        meta_forward.start()
        epick[...] = pick_of(emeta[2 * near + tp_count:2 * near + tp_count + side])[1]

    def pack_end():
        for c in range(PIECES):
            packed = dot(epick[...], eblock[c]).astype(jnp.bfloat16).reshape(side, cap, part_w)
            nrecv[tp_count, :, c * part_w:(c + 1) * part_w] = packed[0]
            for j in range(1, side):
                esend[j, :, c * part_w:(c + 1) * part_w] = packed[j]
        for j in range(1, side):
            eout[j].start()

    def send_lend():
        for copy in lend:
            copy.start()

    def send_lent():
        drain(esend, dense_r.at[len(HOP_BY)])
        for copy in pass_on:
            copy.start()

    def relay_meta(v):
        remote(meta.at[far_meta], rmeta.at[v], meta_s, meta_r.at[v],
               at(across_mid, 0)).wait_recv()
        ranks, weights = rmeta[v, 0:near], rmeta[v, near:]
        if v == 0:
            ranks = jnp.concatenate([ranks[tp_count:], ranks[:tp_count]], axis=0)
            weights = jnp.concatenate([weights[tp_count:], weights[:tp_count]], axis=0)
        rp, rh, rl = onehots(ranks, weights)
        rpick[v] = rp
        rshare_hi[v] = rh
        rshare_lo[v] = rl

    def relay_out(v, c):
        g, lo, count = span(DENSE_BY[v], c)
        if c == lo:
            drain(rblock.at[v, pl.ds(lo, count)], dense_r.at[WAVE_AT[v] + g])
        packed = dot(rpick[v], rblock[v, c]).astype(jnp.bfloat16).reshape(near, cap, part_w)
        frecv[v, c, 0] = packed[0]
        for i in range(1, near):
            fsend[v, c, i] = packed[i]
        for i in list(range(tp_count + side, near)) + list(range(tp_count, tp_count + side)) + crossing[:-1]:
            far_out[v, c, i].start()

    def far_in(v, c, first):
        g, lo, count = span(FAR_BY, c)
        if c == lo:
            drain(frecv.at[v, pl.ds(lo, count), pl.ds(first, tp_count - first)], far_r.at[v, g])
        block = frecv[v, c].reshape(half, part_w)
        more_gate = dot(block, wg[c * part_w:(c + 1) * part_w])
        more_up = dot(block, wu[c * part_w:(c + 1) * part_w])
        gate_acc[...] = more_gate if c == 0 else gate_acc[...] + more_gate
        up_acc[...] = more_up if c == 0 else up_acc[...] + more_up

    def far_result(v, at_relay):
        hidden = hidden_of(gate_acc[...], up_acc[...])
        for lo, hi in GROUPS:
            result = dot(hidden, wd[:, lo * part_w:hi * part_w])
            result = result.astype(jnp.bfloat16).reshape(tp_count, cap, (hi - lo) * part_w)
            for c in range(lo, hi):
                part = result[:, :, (c - lo) * part_w:(c - lo + 1) * part_w]
                if at_relay:
                    rback[v, c, 0] = part[0]
                for j in range(at_relay, tp_count):
                    fres[v, c, j] = part[j]
                for j in crossing[:tp_count - at_relay]:
                    if not at_relay and (c, j) in to_hop and v == 0:
                        to_hop[c, j].start()
                    elif v or c <= (PACED if at_relay else DIRECT):
                        far_ret[v, c, j].start()

    def late_return(c, js=None):
        for j in crossing[side:] if js is None else js:
            far_ret[0, c, j].start()

    def hop_on(c):
        g, lo, count = span(HOP_BY, c)
        if c == lo:
            drain(hop.at[pl.ds(lo, count)], dense_r.at[g])
        from_hop[c].start()

    def combine(high, low, block):
        total = None
        for comb in (high, low):
            term = lax.dot_general(
                comb, block, (((0,), (0,)), ((), ())), preferred_element_type=jnp.float32
            )
            total = term if total is None else total + term
        return total

    def relay_back(v, c):
        g, lo, count = span(BACK_BY[v], c)
        if c == lo:
            drain(rback.at[v, pl.ds(lo, count), pl.ds(1, near - 1)], dense_r.at[WAVE_AT[v] + g])
        block = rback[v, c].reshape(near * cap, part_w)
        rsend[v, c] = combine(rshare_hi[v], rshare_lo[v], block).astype(jnp.bfloat16)
        final[v, c].start()

    def combine_near():
        for p in range(2):
            lo = p * half
            first = p * tp_count + 1 - p
            drain(nback.at[pl.ds(first, tp_count - 1 + p)], io_sem.at[2 + p])
            block = nback[p * tp_count:(p + 1) * tp_count].reshape(half, width)
            part = combine(share_hi[lo:lo + half], share_lo[lo:lo + half], block)
            acc[...] = acc[...] + part if p else part

    def finish(c):
        g, lo, count = span(FINAL_BY, c)
        if c == lo:
            drain(farback.at[pl.ds(lo, count)], io_sem.at[g])
        part = acc[:, c * part_w:(c + 1) * part_w] + farback[c].astype(jnp.float32)
        out_ref[:, c * part_w:(c + 1) * part_w] = part.astype(out_ref.dtype)

    others = range(1, tp_count)
    second = range(tp_count, near)

    def ends_here():
        @pl.when(jnp.logical_not(is_first))
        def _():
            pl.semaphore_wait(ready, tp_count)

    def weights_here():
        for load in loads:
            load.wait()

    @pl.when(is_boundary)
    def _():
        @pl.when(is_first)
        def _():
            send_near(range(AHEAD))

        pack_near(0)
        send_near(range(1, tp_count), 0)
        ends_here()

        @pl.when(jnp.logical_not(is_first))
        def _():
            send_near(range(AHEAD - 1))

        @pl.when(jnp.logical_not(jnp.logical_or(is_first, is_late)))
        def _():
            send_near([AHEAD - 1])

        relay_meta(0)
        last = PIECES - 1
        ahead = PIECES // 2
        for c in range(ahead):
            relay_out(0, c)
            if c == 0:
                weights_here()
                expert_near(0, 1)
                return_near(others)
        end_meta()
        for c in range(ahead - 1):
            forward_end(c)
        for c in range(ahead, PIECES):
            relay_out(0, c)
            forward_end(c - 1)
        forward_end(last)

        @pl.when(is_first)
        def _():
            send_near(range(AHEAD, tp_count))

        @pl.when(jnp.logical_and(jnp.logical_not(is_first), is_late))
        def _():
            send_near([AHEAD - 1])

        relay_meta(1)
        pack_end()
        relay_out(1, 0)
        for c in range(PIECES // 2):
            far_in(0, c, 1)
        relay_out(1, 1)
        for c in range(PIECES // 2, PIECES):
            far_in(0, c, 1)
        far_result(0, 1)
        relay_out(1, 2)
        relay_out(1, 3)
        expert_near(1, 1)
        relay_out(1, 4)
        relay_out(1, 5)
        relay_back(0, 0)
        relay_out(1, 6)
        relay_back(0, 1)
        relay_out(1, 7)
        for c in range(PACED + 1, PIECES):
            late_return(c, crossing[:-1])

        @pl.when(jnp.logical_not(is_first))
        def _():
            send_near(range(AHEAD, tp_count))

        @pl.when(tp < side)
        def _():
            return_near(second)

        @pl.when(tp >= side)
        def _():
            return_near(second[::-1])

        relay_back(0, 2)
        relay_back(0, 3)
        for c in range(last):
            far_in(1, c, 1)
        relay_back(0, 4)
        far_in(1, last, 1)
        far_result(1, 1)
        relay_back(0, 5)

        @pl.when(jnp.logical_not(jnp.logical_and(holds_back, tp % 2 == 0)))
        def _():
            relay_back(0, last - 1)

        @pl.when(jnp.logical_not(holds_back))
        def _():
            relay_back(0, last)

        for c in range(PIECES):
            relay_back(1, c)

        @pl.when(jnp.logical_and(holds_back, tp % 2 == 0))
        def _():
            relay_back(0, last - 1)

        @pl.when(holds_back)
        def _():
            relay_back(0, last)

        combine_near()
        for c in range(PIECES):
            finish(c)

    @pl.when(is_end)
    def _():
        send_lend()
        pack_near(0)
        send_near(range(1, tp_count), 0)
        send_lent()
        weights_here()
        near_part(tp_count, 0, side, 1)
        return_near(list(second)[:EARLY])
        for c in range(PIECES):
            far_in(0, c, 0)
        far_result(0, 0)
        hop_on(3)
        late_return(4)
        late_return(5)
        expert_near(0, 1)
        for c in range(4):
            far_in(1, c, 0)
        hop_on(4)
        hop_on(5)
        late_return(6)
        late_return(7)
        far_in(1, 4, 0)
        far_in(1, 5, 0)
        hop_on(6)
        hop_on(7)
        far_in(1, 6, 0)
        far_in(1, 7, 0)
        far_result(1, 0)
        return_near(others)
        return_near(list(second)[EARLY:side])
        near_part(tp_count + side, 0, tp_count - side, 2)
        return_near(list(second)[side:])
        combine_near()
        for c in range(PIECES):
            finish(c)

    drain(normed, dense_s)
    drain(nres.at[pl.ds(1, near - 1)], w_sem.at[0])

    @pl.when(is_end)
    def _():
        drain(meta, meta_s)
        drain(nsend.at[pl.ds(1, tp_count + side - 1)], near_s)
        drain(esend, eout_s)
        drain(fres, w_sem.at[1])
        drain(hop.at[pl.ds(DIRECT, PIECES - DIRECT)], fwd_s)

    @pl.when(is_boundary)
    def _():
        drain(rmeta, meta_s)
        drain(eblock, fwd_s)
        drain(nsend.at[pl.ds(1, near - 1)], near_s)
        drain(esend.at[pl.ds(1, side - 1)], eout_s)
        drain(fres.at[:, :, pl.ds(1, tp_count - 1)], w_sem.at[1])
        drain(fsend.at[:, :, pl.ds(1, near - 1)], far_s)
        drain(rsend, w_sem.at[2])


def fused(ep_count, tp_count, tokens, norm_gain, route_ids, route_weights, w_gate, w_up, w_down):
    rows, width = tokens.shape
    hidden = w_gate.shape[2]
    experts = ep_count * tp_count
    near = 2 * tp_count
    cap = 3 * rows * route_ids.shape[1] // (2 * experts)
    part_w = width // PIECES
    vmem = pl.BlockSpec(memory_space=pltpu.VMEM)
    hbm = pl.BlockSpec(memory_space=pltpu.HBM)

    def b16(*shape):
        return pltpu.VMEM(shape, jnp.bfloat16)

    def f32(*shape):
        return pltpu.VMEM(shape, jnp.float32)

    def sems(*shape):
        return pltpu.SemaphoreType.DMA(shape)

    one = pltpu.SemaphoreType.DMA
    return pl.pallas_call(
        functools.partial(kernel, ep_count, tp_count, cap),
        out_shape=jax.ShapeDtypeStruct((rows, width), tokens.dtype),
        in_specs=[hbm] * 7,
        out_specs=vmem,
        scratch_shapes=[
            b16(rows, width), f32(1, width),
            pltpu.VMEM(route_ids.shape[::-1], jnp.int32), f32(*route_weights.shape[::-1]), sems(4),
            b16(PIECES, rows, part_w), f32(3 * near, rows),
            b16(near * cap, rows), b16(near * cap, rows),
            *[b16(near, cap, width)] * 4,
            b16(PIECES, rows, part_w), f32(3 * near, rows),
            b16(tp_count // 2 * cap, rows), b16(tp_count // 2, cap, width),
            b16(PIECES, tp_count // 2, cap, part_w),
            b16(2, PIECES, rows, part_w), f32(2, 2 * near, rows),
            *[b16(2, near * cap, rows)] * 3,
            b16(2, PIECES, near, cap, part_w),
            b16(2, PIECES, tp_count, cap, part_w),
            b16(2, PIECES, tp_count, cap, part_w),
            b16(2, PIECES, near, cap, part_w),
            b16(2, PIECES, rows, part_w), b16(PIECES, rows, part_w),
            b16(width, hidden), b16(width, hidden), b16(hidden, width),
            f32(rows, width), f32(tp_count * cap, hidden), f32(tp_count * cap, hidden),
            sems(3), pltpu.SemaphoreType.REGULAR, one, one,
            sems(len(EDENSE_BY) - 1), sems(sum(map(len, DENSE_BY)) - 2),
            one, sems(1), sems(2), one, sems(3), one, one, sems(2, len(FAR_BY) - 1),
        ],
        compiler_params=pltpu.CompilerParams(
            collective_id=0, has_side_effects=True, vmem_limit_bytes=32 * 1024 * 1024
        ),
    )(*(
        pltpu.with_memory_space_constraint(arg, pltpu.HBM)
        for arg in (tokens, norm_gain.reshape(1, width), route_ids.T, route_weights.T,
                    w_gate, w_up, w_down)
    ))


def solution(mesh):
    ep_count, tp_count = mesh.shape["ep"], mesh.shape["tp"]

    def on_device(*args):
        rows, experts = args[0].shape[0], ep_count * tp_count
        cap = 3 * rows * args[2].shape[1] // (2 * experts)
        if ep_count != 4 or tp_count != 4 or cap % 8 or rows % 128 or args[0].shape[1] % 256:
            return plain(*args)
        return fused(ep_count, tp_count, *args)

    return jax.shard_map(
        on_device,
        mesh=mesh,
        in_specs=(
            P(("grp", "ep", "tp"), None),
            P(),
            P(("grp", "ep", "tp"), None),
            P(("grp", "ep", "tp"), None),
            P(("ep", "tp"), None, None),
            P(("ep", "tp"), None, None),
            P(("ep", "tp"), None, None),
        ),
        out_specs=P(("grp", "ep", "tp"), None),
        check_vma=False,
    )
```

```python
import functools

import jax
import jax.numpy as jnp
from jax import lax
from jax.experimental import pallas as pl
from jax.experimental.pallas import tpu as pltpu
from jax.sharding import PartitionSpec as P

MESH = pl.DeviceIdType.MESH


def plain(tokens, norm_gain, route_ids, route_weights, w_gate, w_up, w_down):
    tok_rows, model_width = tokens.shape
    top_count = route_ids.shape[1]
    ep_count = lax.axis_size("ep")
    tp_count = lax.axis_size("tp")
    experts = ep_count * tp_count
    capacity = 3 * tok_rows * top_count // (2 * experts)
    values = tokens.astype(jnp.float32)
    normed = (
        values * lax.rsqrt(jnp.mean(values * values, axis=-1, keepdims=True) + 1e-06) * norm_gain
    ).astype(jnp.bfloat16)
    flat_ids = route_ids.reshape(-1)
    onehot = (flat_ids[:, None] == jnp.arange(experts, dtype=jnp.int32)[None, :]).astype(jnp.int32)
    slot_index = jnp.sum((jnp.cumsum(onehot, axis=0) - onehot) * onehot, axis=-1)
    token_of = jnp.arange(tok_rows * top_count, dtype=jnp.int32) // top_count
    buffer = jnp.zeros((experts, capacity, model_width), jnp.bfloat16)
    buffer = buffer.at[flat_ids, slot_index].set(normed[token_of])
    received = lax.all_to_all(buffer, ("ep", "tp"), split_axis=0, concat_axis=0, tiled=True)
    flat_rows = received.reshape(-1, model_width)
    gate_act = jnp.dot(flat_rows, w_gate[0], preferred_element_type=jnp.float32)
    up_act = jnp.dot(flat_rows, w_up[0], preferred_element_type=jnp.float32)
    hidden = (jax.nn.silu(gate_act) * up_act).astype(jnp.bfloat16)
    result = jnp.dot(hidden, w_down[0], preferred_element_type=jnp.float32).astype(jnp.bfloat16)
    returned = lax.all_to_all(
        result.reshape(received.shape), ("ep", "tp"), split_axis=0, concat_axis=0, tiled=True
    )
    picked = (
        returned[flat_ids, slot_index].reshape(tok_rows, top_count, model_width).astype(jnp.float32)
    )
    return jnp.sum(picked * route_weights[:, :, None], axis=1).astype(jnp.bfloat16)


def flipped(index, bits):
    bit = 1
    while bit <= bits:
        if bits & bit:
            index = index + (1 - 2 * ((index // bit) % 2)) * bit
        bit *= 2
    return index


PIECES = 8
EARLY = 1
AHEAD = 3
DIRECT = 3
PACED = 3
GROUPS = ((0, 1), (1, 3), (3, 8))
DENSE_BY = ((0, 2, 3, 4, 5, 6, 7, 8), (0, 1, 2, 3, 4, 5, 6, 7, 8))
EDENSE_BY = (0, 4, 6, 8)
FAR_BY = (0, 4, 6, 7, 8)
BACK_BY = ((0, 1, 2, 3, 4, 5, 6, 8), (0, 1, 2, 3, 4, 5, 6, 7, 8))
HOP_BY = (DIRECT, 4, 6, 8)
FINAL_BY = (0, 7, 8)
WAVE_AT = (0, len(DENSE_BY[0]) - 1)


def span(edges, c):
    g = max(i for i in range(len(edges) - 1) if edges[i] <= c)
    return g, edges[g], edges[g + 1] - edges[g]


def slot(edges, c):
    return span(edges, c)[0]


def kernel(
    ep_count, tp_count, cap,
    x_hbm, gain_hbm, ids_hbm, wts_hbm, wg_hbm, wu_hbm, wd_hbm, out_ref,
    x_ref, gain_ref, ids_ref, wts_ref, io_sem,
    normed, meta, share_hi, share_lo, nsend, nrecv, nres, nback,
    eblock, emeta, epick, esend, hop,
    rblock, rmeta, rpick, rshare_hi, rshare_lo, fsend, frecv, fres, rback, rsend, farback,
    wg, wu, wd, acc, gate_acc, up_acc,
    w_sem, ready, dense_s, fwd_s, edense_r, dense_r, meta_s, emeta_r, meta_r, near_s, near_r,
    eout_s, far_s, far_r,
):
    ep, tp, grp = lax.axis_index("ep"), lax.axis_index("tp"), lax.axis_index("grp")
    rows, width = x_ref.shape
    part_w = width // PIECES
    top = ids_ref.shape[0]
    experts = ep_count * tp_count
    near = 2 * tp_count
    me = ep * tp_count + tp
    boundary = (ep + ep // 2) % 2
    place_of_me = (1 - boundary) * tp_count
    own_relay = 1 + ep // 2
    is_boundary, is_end = boundary == 1, boundary == 0
    is_first = ep < ep_count // 2
    is_late = tp % 2 == 1
    holds_back = ep == ep_count // 2

    def at(plane, j):
        return (grp, plane, flipped(tp, j))

    def remote(src, dst, s_sem, r_sem, target):
        return pltpu.make_async_remote_copy(
            src_ref=src, dst_ref=dst, send_sem=s_sem, recv_sem=r_sem,
            device_id=target, device_id_type=MESH,
        )

    barrier = pltpu.get_barrier_semaphore()

    def greet(target):
        pl.semaphore_signal(barrier, inc=1, device_id=target, device_id_type=MESH)

    @pl.when(is_boundary)
    def _():
        greet(at(flipped(ep, 3), 0))
        for j in range(tp_count):
            greet(at(flipped(ep, 1), j))

    @pl.when(jnp.logical_and(is_end, is_first))
    def _():
        for j in range(tp_count):
            greet(at(flipped(ep, 1), j))

    for j in range(1, tp_count):
        greet(at(ep, j))
    fetches = [
        pltpu.make_async_copy(src, dst, io_sem.at[i])
        for i, (src, dst) in enumerate((
            (x_hbm, x_ref), (gain_hbm, gain_ref), (ids_hbm, ids_ref), (wts_hbm, wts_ref)))
    ]
    for fetch in fetches:
        fetch.start()
    loads = [
        pltpu.make_async_copy(src.at[0], dst, w_sem.at[i])
        for i, (src, dst) in enumerate(((wg_hbm, wg), (wu_hbm, wu), (wd_hbm, wd)))
    ]
    partner, across_mid = flipped(ep, 1), flipped(ep, 3)

    @pl.when(is_end)
    def _():
        pl.semaphore_wait(barrier, near - 1)

    @pl.when(jnp.logical_and(is_end, jnp.logical_not(is_first)))
    def _():
        for j in range(tp_count):
            pl.semaphore_signal(ready, inc=1, device_id=at(partner, j), device_id_type=MESH)

    planes = [ep, partner]
    dense = [
        remote(normed.at[c], rblock.at[0, c], dense_s, dense_r.at[slot(DENSE_BY[0], c)], at(across_mid, 0))
        for c in range(PIECES)
    ]
    forward = [
        remote(eblock.at[c], rblock.at[1, c], fwd_s, dense_r.at[WAVE_AT[1] + slot(DENSE_BY[1], c)], at(across_mid, 0))
        for c in range(PIECES)
    ]
    edense = [
        remote(normed.at[c], eblock.at[c], dense_s, edense_r.at[slot(EDENSE_BY, c)], at(partner, 0))
        for c in range(PIECES)
    ]
    far_meta = pl.ds(0, 2 * near)
    meta_copy = remote(meta.at[far_meta], rmeta.at[0], meta_s, meta_r.at[0],
                       at(across_mid, 0))
    meta_forward = remote(emeta.at[far_meta], rmeta.at[1], meta_s, meta_r.at[1],
                          at(across_mid, 0))
    emeta_copy = remote(meta, emeta, meta_s, emeta_r.at[0], at(partner, 0))
    near_out = [
        remote(nsend.at[g], nrecv.at[g], near_s, near_r.at[max(0, 2 * g // tp_count - 1)],
               at(planes[g // tp_count], g % tp_count))
        for g in range(near)
    ]
    side = tp_count // 2
    eout = [
        remote(esend.at[j], nrecv.at[tp_count + j], eout_s, near_r.at[1], at(ep, j))
        for j in range(side)
    ]
    lend = [
        remote(nsend.at[tp_count + side + k], esend.at[k], near_s, dense_r.at[len(HOP_BY)], at(ep, side))
        for k in range(side)
    ]
    pass_on = [
        remote(esend.at[k], nrecv.at[tp_count + side + k], eout_s, near_r.at[1], at(partner, k))
        for k in range(side)
    ]
    near_ret = [
        remote(nres.at[g], nback.at[g], w_sem.at[0], io_sem.at[2 + g // tp_count],
               at(planes[g // tp_count], g % tp_count))
        for g in range(near)
    ]
    far_out, far_ret, to_hop, from_hop, final = {}, {}, {}, {}, {}
    for v in range(2):
        for c in range(PIECES):
            for i in range(near):
                far_out[v, c, i] = remote(
                    fsend.at[v, c, i], frecv.at[v, c, i % tp_count], far_s,
                    far_r.at[v, slot(FAR_BY, c)], at(planes[i // tp_count], i % tp_count))
            for j in range(tp_count):
                place = place_of_me + j
                far_ret[v, c, j] = remote(
                    fres.at[v, c, j], rback.at[v, c, place], w_sem.at[1], dense_r.at[WAVE_AT[v] + slot(BACK_BY[v], c)],
                    at(own_relay, j))
            if v == 0 and c >= DIRECT:
                for j in range(side, tp_count):
                    to_hop[c, j] = remote(fres.at[v, c, j], hop.at[c, j - side], w_sem.at[1],
                                          dense_r.at[slot(HOP_BY, c)], at(ep, j))
                from_hop[c] = remote(hop.at[c], rback.at[v, c, pl.ds(tp_count + side, side)],
                                     fwd_s, dense_r.at[WAVE_AT[v] + slot(BACK_BY[v], c)], at(own_relay, 0))
            final[v, c] = remote(rsend.at[v, c], farback.at[c], w_sem.at[2], io_sem.at[slot(FINAL_BY, c)],
                                 at(flipped(ep, 3 - v), 0))

    def drain(ref, sem):
        pltpu.make_async_copy(ref, ref, sem).wait()

    for fetch in fetches[:2]:
        fetch.wait()
    for load in loads:
        load.start()
    values = x_ref[...].astype(jnp.float32)
    rows_normed = (
        values
        * lax.rsqrt(jnp.mean(values * values, axis=-1, keepdims=True) + 1e-06)
        * gain_ref[...]
    ).astype(jnp.bfloat16)
    for c in range(PIECES):
        normed[c] = rows_normed[:, c * part_w:(c + 1) * part_w]

    @pl.when(is_boundary)
    def _():
        pl.semaphore_wait(barrier, tp_count + jnp.where(is_first, tp_count, 0))
        for c in range(2):
            dense[c].start()

    @pl.when(is_end)
    def _():
        for c in range(2):
            edense[c].start()

    down = lax.broadcasted_iota(jnp.int32, (rows, rows), 0)
    across = lax.broadcasted_iota(jnp.int32, (rows, rows), 1)

    expert_of = lax.broadcasted_iota(jnp.int32, (experts, rows), 0) ^ me
    for fetch in fetches[2:]:
        fetch.wait()
    ids, wts = ids_ref[...], wts_ref[...]
    named = jnp.zeros((experts, rows), jnp.float32)
    weight = jnp.zeros((experts, rows), jnp.float32)
    for k in range(top):
        match = ids[k:k + 1] == expert_of
        named = named + jnp.where(match, 1.0, 0.0)
        weight = weight + jnp.where(match, wts[k:k + 1], 0.0)
    earlier = jnp.where(down < across, 1.0, 0.0).astype(jnp.bfloat16)
    rank = jnp.dot(named.astype(jnp.bfloat16), earlier, preferred_element_type=jnp.float32)
    rank = jnp.where(named > 0.5, rank, -1.0)
    meta[0:near] = rank[near:]
    meta[near:2 * near] = weight[near:]
    meta[2 * near:] = rank[:near]

    @pl.when(is_boundary)
    def _():
        meta_copy.start()
        for c in range(2, PIECES):
            dense[c].start()

    @pl.when(is_end)
    def _():
        emeta_copy.start()
        for c in range(2, PIECES):
            edense[c].start()

    def pick_of(rank):
        count = rank.shape[0]
        slot = lax.broadcasted_iota(jnp.int32, (count, cap, rows), 1).astype(jnp.float32)
        taken = rank[:, None, :] == slot
        pick = jnp.where(taken, 1.0, 0.0).reshape(count * cap, rows).astype(jnp.bfloat16)
        return taken, pick

    def onehots(rank, weight):
        taken, pick = pick_of(rank)
        share = jnp.where(taken, weight[:, None, :], 0.0).reshape(near * cap, rows)
        high = share.astype(jnp.bfloat16)
        return pick, high, (share - high.astype(jnp.float32)).astype(jnp.bfloat16)

    pick, high, low = onehots(rank[:near], weight[:near])

    def dot(a, b):
        return jnp.dot(a, b, preferred_element_type=jnp.float32)

    half = tp_count * cap
    crossing = [*range(side, tp_count), *range(side - 1, -1, -1)]

    def pack_near(p):
        packed = dot(pick[p * half:(p + 1) * half], rows_normed)
        packed = packed.astype(jnp.bfloat16).reshape(tp_count, cap, width)
        for j in range(tp_count):
            if p or j:
                nsend[p * tp_count + j] = packed[j]
            else:
                nrecv[0] = packed[0]

    pack_near(1)

    share_hi[...] = high
    share_lo[...] = low

    def send_near(js, p=1):
        for j in js:
            near_out[p * tp_count + j].start()

    def hidden_of(gate_act, up_act):
        return (gate_act / (1.0 + jnp.exp(-gate_act)) * up_act).astype(jnp.bfloat16)

    def near_part(base, first, count, sem):
        drain(nrecv.at[pl.ds(base + first, count - first)], near_r.at[sem])
        block = nrecv[base:base + count].reshape(count * cap, width)
        hidden = hidden_of(dot(block, wg[...]), dot(block, wu[...]))
        result = dot(hidden, wd[...]).astype(jnp.bfloat16).reshape(count, cap, width)
        for j in range(count):
            if base or j:
                nres[base + j] = result[j]
            else:
                nback[0] = result[0]

    def expert_near(p, first):
        near_part(p * tp_count, first, tp_count, p)

    def return_near(gs):
        for g in gs:
            near_ret[g].start()

    def forward_end(c):
        g, lo, count = span(EDENSE_BY, c)
        if c == lo:
            drain(eblock.at[pl.ds(lo, count)], edense_r.at[g])
        forward[c].start()

    def end_meta():
        emeta_copy.wait_recv()
        meta_forward.start()
        epick[...] = pick_of(emeta[2 * near + tp_count:2 * near + tp_count + side])[1]

    def pack_end():
        for c in range(PIECES):
            packed = dot(epick[...], eblock[c]).astype(jnp.bfloat16).reshape(side, cap, part_w)
            nrecv[tp_count, :, c * part_w:(c + 1) * part_w] = packed[0]
            for j in range(1, side):
                esend[j, :, c * part_w:(c + 1) * part_w] = packed[j]
        for j in range(1, side):
            eout[j].start()

    def send_lend():
        for copy in lend:
            copy.start()

    def send_lent():
        drain(esend, dense_r.at[len(HOP_BY)])
        for copy in pass_on:
            copy.start()

    def relay_meta(v):
        remote(meta.at[far_meta], rmeta.at[v], meta_s, meta_r.at[v],
               at(across_mid, 0)).wait_recv()
        ranks, weights = rmeta[v, 0:near], rmeta[v, near:]
        if v == 0:
            ranks = jnp.concatenate([ranks[tp_count:], ranks[:tp_count]], axis=0)
            weights = jnp.concatenate([weights[tp_count:], weights[:tp_count]], axis=0)
        rp, rh, rl = onehots(ranks, weights)
        rpick[v] = rp
        rshare_hi[v] = rh
        rshare_lo[v] = rl

    def relay_out(v, c):
        g, lo, count = span(DENSE_BY[v], c)
        if c == lo:
            drain(rblock.at[v, pl.ds(lo, count)], dense_r.at[WAVE_AT[v] + g])
        packed = dot(rpick[v], rblock[v, c]).astype(jnp.bfloat16).reshape(near, cap, part_w)
        frecv[v, c, 0] = packed[0]
        for i in range(1, near):
            fsend[v, c, i] = packed[i]
        for i in list(range(tp_count + side, near)) + list(range(tp_count, tp_count + side)) + crossing[:-1]:
            far_out[v, c, i].start()

    def far_in(v, c, first):
        g, lo, count = span(FAR_BY, c)
        if c == lo:
            drain(frecv.at[v, pl.ds(lo, count), pl.ds(first, tp_count - first)], far_r.at[v, g])
        block = frecv[v, c].reshape(half, part_w)
        more_gate = dot(block, wg[c * part_w:(c + 1) * part_w])
        more_up = dot(block, wu[c * part_w:(c + 1) * part_w])
        gate_acc[...] = more_gate if c == 0 else gate_acc[...] + more_gate
        up_acc[...] = more_up if c == 0 else up_acc[...] + more_up

    def far_result(v, at_relay):
        hidden = hidden_of(gate_acc[...], up_acc[...])
        for lo, hi in GROUPS:
            result = dot(hidden, wd[:, lo * part_w:hi * part_w])
            result = result.astype(jnp.bfloat16).reshape(tp_count, cap, (hi - lo) * part_w)
            for c in range(lo, hi):
                part = result[:, :, (c - lo) * part_w:(c - lo + 1) * part_w]
                if at_relay:
                    rback[v, c, 0] = part[0]
                for j in range(at_relay, tp_count):
                    fres[v, c, j] = part[j]
                for j in crossing[:tp_count - at_relay]:
                    if not at_relay and (c, j) in to_hop and v == 0:
                        to_hop[c, j].start()
                    elif v or c <= (PACED if at_relay else DIRECT):
                        far_ret[v, c, j].start()

    def late_return(c, js=None):
        for j in crossing[side:] if js is None else js:
            far_ret[0, c, j].start()

    def hop_on(c):
        g, lo, count = span(HOP_BY, c)
        if c == lo:
            drain(hop.at[pl.ds(lo, count)], dense_r.at[g])
        from_hop[c].start()

    def combine(high, low, block):
        total = None
        for comb in (high, low):
            term = lax.dot_general(
                comb, block, (((0,), (0,)), ((), ())), preferred_element_type=jnp.float32
            )
            total = term if total is None else total + term
        return total

    def relay_back(v, c):
        g, lo, count = span(BACK_BY[v], c)
        if c == lo:
            drain(rback.at[v, pl.ds(lo, count), pl.ds(1, near - 1)], dense_r.at[WAVE_AT[v] + g])
        block = rback[v, c].reshape(near * cap, part_w)
        rsend[v, c] = combine(rshare_hi[v], rshare_lo[v], block).astype(jnp.bfloat16)
        final[v, c].start()

    def combine_part(p):
        lo = p * half
        first = p * tp_count + 1 - p
        drain(nback.at[pl.ds(first, tp_count - 1 + p)], io_sem.at[2 + p])
        block = nback[p * tp_count:(p + 1) * tp_count].reshape(half, width)
        return combine(share_hi[lo:lo + half], share_lo[lo:lo + half], block)

    def arrived(c):
        g, lo, count = span(FINAL_BY, c)
        if c == lo:
            drain(farback.at[pl.ds(lo, count)], io_sem.at[g])

    def finish_all():
        acc[...] = combine_part(0)
        part = combine_part(1)
        tail = (PIECES - 1) * part_w
        for c in range(PIECES - 1):
            arrived(c)
            cols = slice(c * part_w, (c + 1) * part_w)
            total = acc[:, cols] + part[:, cols] + farback[c].astype(jnp.float32)
            out_ref[:, cols] = total.astype(out_ref.dtype)
        acc[:, tail:] = acc[:, tail:] + part[:, tail:]
        arrived(PIECES - 1)
        total = acc[:, tail:] + farback[PIECES - 1].astype(jnp.float32)
        out_ref[:, tail:] = total.astype(out_ref.dtype)

    others = range(1, tp_count)
    second = range(tp_count, near)

    def ends_here():
        @pl.when(jnp.logical_not(is_first))
        def _():
            pl.semaphore_wait(ready, tp_count)

    def weights_here():
        for load in loads:
            load.wait()

    @pl.when(is_boundary)
    def _():
        @pl.when(is_first)
        def _():
            send_near(range(AHEAD))

        pack_near(0)
        send_near(range(1, tp_count), 0)
        ends_here()

        @pl.when(jnp.logical_not(is_first))
        def _():
            send_near(range(AHEAD - 1))

        @pl.when(jnp.logical_not(jnp.logical_or(is_first, is_late)))
        def _():
            send_near([AHEAD - 1])

        relay_meta(0)
        last = PIECES - 1
        ahead = PIECES // 2
        for c in range(ahead):
            relay_out(0, c)
            if c == 0:
                weights_here()
                expert_near(0, 1)
                return_near(others)
        end_meta()
        for c in range(ahead - 1):
            forward_end(c)
        for c in range(ahead, PIECES):
            relay_out(0, c)
            forward_end(c - 1)
        forward_end(last)

        @pl.when(is_first)
        def _():
            send_near(range(AHEAD, tp_count))

        @pl.when(jnp.logical_and(jnp.logical_not(is_first), is_late))
        def _():
            send_near([AHEAD - 1])

        relay_meta(1)
        pack_end()
        relay_out(1, 0)
        for c in range(PIECES // 2):
            far_in(0, c, 1)
        relay_out(1, 1)
        for c in range(PIECES // 2, PIECES):
            far_in(0, c, 1)
        far_result(0, 1)
        relay_out(1, 2)
        relay_out(1, 3)
        expert_near(1, 1)
        relay_out(1, 4)
        relay_out(1, 5)
        relay_back(0, 0)
        relay_out(1, 6)
        relay_back(0, 1)
        relay_out(1, 7)
        for c in range(PACED + 1, PIECES):
            late_return(c, crossing[:-1])

        @pl.when(jnp.logical_not(is_first))
        def _():
            send_near(range(AHEAD, tp_count))

        @pl.when(tp < side)
        def _():
            return_near(second)

        @pl.when(tp >= side)
        def _():
            return_near(second[::-1])

        relay_back(0, 2)
        relay_back(0, 3)
        for c in range(last):
            far_in(1, c, 1)
        relay_back(0, 4)
        far_in(1, last, 1)
        far_result(1, 1)
        relay_back(0, 5)

        @pl.when(jnp.logical_not(jnp.logical_and(holds_back, tp % 2 == 0)))
        def _():
            relay_back(0, last - 1)

        @pl.when(jnp.logical_not(holds_back))
        def _():
            relay_back(0, last)

        for c in range(PIECES):
            relay_back(1, c)

        @pl.when(jnp.logical_and(holds_back, tp % 2 == 0))
        def _():
            relay_back(0, last - 1)

        @pl.when(holds_back)
        def _():
            relay_back(0, last)

        finish_all()

    @pl.when(is_end)
    def _():
        send_lend()
        pack_near(0)
        send_near(range(1, tp_count), 0)
        send_lent()
        weights_here()
        near_part(tp_count, 0, side, 1)
        return_near(list(second)[:EARLY])
        for c in range(PIECES):
            far_in(0, c, 0)
        far_result(0, 0)
        hop_on(3)
        late_return(4)
        late_return(5)
        expert_near(0, 1)
        for c in range(4):
            far_in(1, c, 0)
        hop_on(4)
        hop_on(5)
        late_return(6)
        late_return(7)
        far_in(1, 4, 0)
        far_in(1, 5, 0)
        hop_on(6)
        hop_on(7)
        far_in(1, 6, 0)
        far_in(1, 7, 0)
        far_result(1, 0)
        return_near(others)
        return_near(list(second)[EARLY:side])
        near_part(tp_count + side, 0, tp_count - side, 2)
        return_near(list(second)[side:])
        finish_all()

    drain(normed, dense_s)
    drain(nres.at[pl.ds(1, near - 1)], w_sem.at[0])

    @pl.when(is_end)
    def _():
        drain(meta, meta_s)
        drain(nsend.at[pl.ds(1, tp_count + side - 1)], near_s)
        drain(esend, eout_s)
        drain(fres, w_sem.at[1])
        drain(hop.at[pl.ds(DIRECT, PIECES - DIRECT)], fwd_s)

    @pl.when(is_boundary)
    def _():
        drain(rmeta, meta_s)
        drain(eblock, fwd_s)
        drain(nsend.at[pl.ds(1, near - 1)], near_s)
        drain(esend.at[pl.ds(1, side - 1)], eout_s)
        drain(fres.at[:, :, pl.ds(1, tp_count - 1)], w_sem.at[1])
        drain(fsend.at[:, :, pl.ds(1, near - 1)], far_s)
        drain(rsend, w_sem.at[2])


def fused(ep_count, tp_count, tokens, norm_gain, route_ids, route_weights, w_gate, w_up, w_down):
    rows, width = tokens.shape
    hidden = w_gate.shape[2]
    experts = ep_count * tp_count
    near = 2 * tp_count
    cap = 3 * rows * route_ids.shape[1] // (2 * experts)
    part_w = width // PIECES
    vmem = pl.BlockSpec(memory_space=pltpu.VMEM)
    hbm = pl.BlockSpec(memory_space=pltpu.HBM)

    def b16(*shape):
        return pltpu.VMEM(shape, jnp.bfloat16)

    def f32(*shape):
        return pltpu.VMEM(shape, jnp.float32)

    def sems(*shape):
        return pltpu.SemaphoreType.DMA(shape)

    one = pltpu.SemaphoreType.DMA
    return pl.pallas_call(
        functools.partial(kernel, ep_count, tp_count, cap),
        out_shape=jax.ShapeDtypeStruct((rows, width), tokens.dtype),
        in_specs=[hbm] * 7,
        out_specs=vmem,
        scratch_shapes=[
            b16(rows, width), f32(1, width),
            pltpu.VMEM(route_ids.shape[::-1], jnp.int32), f32(*route_weights.shape[::-1]), sems(4),
            b16(PIECES, rows, part_w), f32(3 * near, rows),
            b16(near * cap, rows), b16(near * cap, rows),
            *[b16(near, cap, width)] * 4,
            b16(PIECES, rows, part_w), f32(3 * near, rows),
            b16(tp_count // 2 * cap, rows), b16(tp_count // 2, cap, width),
            b16(PIECES, tp_count // 2, cap, part_w),
            b16(2, PIECES, rows, part_w), f32(2, 2 * near, rows),
            *[b16(2, near * cap, rows)] * 3,
            b16(2, PIECES, near, cap, part_w),
            b16(2, PIECES, tp_count, cap, part_w),
            b16(2, PIECES, tp_count, cap, part_w),
            b16(2, PIECES, near, cap, part_w),
            b16(2, PIECES, rows, part_w), b16(PIECES, rows, part_w),
            b16(width, hidden), b16(width, hidden), b16(hidden, width),
            f32(rows, width), f32(tp_count * cap, hidden), f32(tp_count * cap, hidden),
            sems(3), pltpu.SemaphoreType.REGULAR, one, one,
            sems(len(EDENSE_BY) - 1), sems(sum(map(len, DENSE_BY)) - 2),
            one, sems(1), sems(2), one, sems(3), one, one, sems(2, len(FAR_BY) - 1),
        ],
        compiler_params=pltpu.CompilerParams(
            collective_id=0, has_side_effects=True, vmem_limit_bytes=32 * 1024 * 1024
        ),
    )(*(
        pltpu.with_memory_space_constraint(arg, pltpu.HBM)
        for arg in (tokens, norm_gain.reshape(1, width), route_ids.T, route_weights.T,
                    w_gate, w_up, w_down)
    ))


def solution(mesh):
    ep_count, tp_count = mesh.shape["ep"], mesh.shape["tp"]

    def on_device(*args):
        rows, experts = args[0].shape[0], ep_count * tp_count
        cap = 3 * rows * args[2].shape[1] // (2 * experts)
        if ep_count != 4 or tp_count != 4 or cap % 8 or rows % 128 or args[0].shape[1] % 256:
            return plain(*args)
        return fused(ep_count, tp_count, *args)

    return jax.shard_map(
        on_device,
        mesh=mesh,
        in_specs=(
            P(("grp", "ep", "tp"), None),
            P(),
            P(("grp", "ep", "tp"), None),
            P(("grp", "ep", "tp"), None),
            P(("ep", "tp"), None, None),
            P(("ep", "tp"), None, None),
            P(("ep", "tp"), None, None),
        ),
        out_specs=P(("grp", "ep", "tp"), None),
        check_vma=False,
    )
```
